256 devices in a mesh: ep: 64 (over z, x, core), tp: 4 (over y).
Axes of the slice: x: 4, y: 4, z: 8, core: 2. Of those that a mesh axis runs over, the one named last changes fastest.
Arguments:
- query_latent: bfloat16 [8192, 512], P('ep'), may hold values from -6 to 6
- key_latent: bfloat16 [8192, 256], P('ep'), may hold values from -6 to 6
- rope_key: bfloat16 [8192, 64], P('ep'), may hold values from -500 to 500
- query_gain: float32 [512], replicated, may hold values from 0.1 to 1.9
- key_gain: float32 [256], replicated, may hold values from 0.1 to 1.9
- w_query: bfloat16 [512, 1024], P(None, 'tp'), may hold values from -0.25 to 0.25
- w_query_rope: bfloat16 [512, 512], P(None, 'tp'), may hold values from -0.25 to 0.25
- w_key: bfloat16 [256, 1024], P(None, 'tp'), may hold values from -0.375 to 0.375
- w_value: bfloat16 [256, 1024], P(None, 'tp'), may hold values from -0.375 to 0.375
- w_out: bfloat16 [1024, 2048], P('tp'), may hold values from -1.796875 to 1.796875
- tokens_b: bfloat16 [32768, 2048], P('ep'), may hold values from -6 to 6
- ffn_gain: float32 [2048], replicated, may hold values from 0.1 to 1.9
- route_expert: int32 [32768, 2], P('ep'), may hold values from 0 to 63, as said below
- route_weight: float32 [32768, 2], P('ep'), may hold values from 0.2 to 1
- w_gate: bfloat16 [64, 2048, 1024], P('ep', None, 'tp'), may hold values from -0.125 to 0.125
- w_up: bfloat16 [64, 2048, 1024], P('ep', None, 'tp'), may hold values from -0.125 to 0.125
- w_down: bfloat16 [64, 1024, 2048], P('ep', 'tp'), may hold values from -0.1875 to 0.1875
Outputs:
- mixer_out: bfloat16 [8192, 2048], P(('ep', 'tp'))
- moe_out: bfloat16 [32768, 2048], P('ep', 'tp')
The draws below stay inside these ranges and needn't reach their ends.
Inputs may be any that keep to these rules, and one draw needn't show every extreme that they name: `route_expert`: expert e belongs to group e // 16. A row's 2 experts differ and lie in one group. Among the rows of one device along ep, every group is named by exactly 128 rows and every expert is named exactly 16 times.
All inputs are finite; a program needn't handle non-finite values.
Results may differ from the reference program's by a relative error of at most 0.013.
The reference program's roundings to bfloat16 on the way count: a program that leaves them out, or rounds other values in their place, can miss the bound.
Values may be sent and summed in bfloat16 or wider, within the bound.
A program may use at most 64 MiB of HBM per device.

```python
import math
import jax
import jax.numpy as jnp
from jax import lax

D = 2048
HEADS = 8
NOPE = 128
ROPE = 64
VDIM = 128
QRANK = 512
KVRANK = 256
GRID_W = 64
FF_E = 1024
GROUPS = 4
TOPK = 2
TOK_A = 128
TOK_B = 512
EXPERTS = 64
TOKENS_A = 8192
TOKENS_B = 32768
N_EP = 64
N_TP = 4


def draw_rope_key(key, part):
    seq_len = TOK_A * N_EP
    key_base = jax.random.fold_in(key, 0)
    return jnp.clip(3.0 * jax.random.normal(key_base, (seq_len, ROPE), jnp.float32), -18.0, 18.0).astype(jnp.bfloat16)


def draw_route_expert(key, part):
    group_rows = TOK_B // GROUPS
    in_group = EXPERTS // GROUPS
    key_order, key_rotation, key_shift = jax.random.split(key, 3)
    ranking = jax.random.randint(key_order, (N_EP, TOK_B), 0, 1 << 16) * TOK_B + jnp.arange(TOK_B, dtype=jnp.int32)[None, :]
    ordering = jnp.argsort(ranking, axis=1, stable=True)
    position = jnp.argsort(ordering, axis=1, stable=True).astype(jnp.int32)
    group_of = position // group_rows
    within = position % group_rows
    rotation = jax.random.randint(key_rotation, (N_EP, GROUPS), 0, in_group)
    shifted = jax.random.randint(key_shift, (N_EP, GROUPS), 1, in_group)
    rotation_row = jnp.take_along_axis(rotation, group_of, axis=1)
    shift_row = jnp.take_along_axis(shifted, group_of, axis=1)
    first_choice = group_of * in_group + (within + rotation_row) % in_group
    second_choice = group_of * in_group + (within + rotation_row + shift_row) % in_group
    routes = jnp.stack([first_choice, second_choice], axis=-1)
    return routes.reshape(N_EP * TOK_B, TOPK).astype(jnp.int32)


def levels(key, extent, pieces, smallest, top_value):
    loudness = 1.0
    for dim, shards_of in pieces:
        draws = jax.random.uniform(jax.random.fold_in(jax.random.fold_in(key, 6), dim), (shards_of,), jnp.float32, smallest / len(pieces), top_value / len(pieces))
        loudness = loudness * jnp.repeat(jnp.exp(draws), extent[dim] // shards_of).reshape((-1,) + (1,) * (len(extent) - 1 - dim))
    return loudness


def noise(stream_key, shape, deviation, most, cuts=(), held_as=jnp.bfloat16):
    values = jax.random.normal(stream_key, shape, jnp.float32) * deviation
    if len(cuts) > 0:
        values = levels(stream_key, shape, cuts, -0.22, 0.18) * values
    return jnp.clip(values, min=-most, max=most).astype(held_as)


def setup_inputs(seed: int = 0) -> dict:
    key_of = jax.random.split(jax.random.key(seed), 18)
    query_latent = noise(key_of[0], (TOKENS_A, QRANK), 1.0, 6.0, ((0, 64),))
    key_latent = noise(key_of[1], (TOKENS_A, KVRANK), 1.0, 6.0, ((0, 64),))
    rope_key = draw_rope_key(jax.random.fold_in(key_of[17], 71), 0)
    query_gain = jnp.clip(1.0 + 0.18 * jax.random.normal(key_of[3], (QRANK,), jnp.float32), 0.1, 1.9)
    key_gain = jnp.clip(1.0 + 0.18 * jax.random.normal(key_of[4], (KVRANK,), jnp.float32), 0.1, 1.9)
    w_query = noise(key_of[5], (QRANK, HEADS * NOPE), QRANK ** -0.5, 0.25, ((1, 4),))
    w_query_rope = noise(key_of[6], (QRANK, HEADS * ROPE), QRANK ** -0.5, 0.25, ((1, 4),))
    w_key = noise(key_of[7], (KVRANK, HEADS * NOPE), KVRANK ** -0.5, 0.375, ((1, 4),))
    w_value = noise(key_of[8], (KVRANK, HEADS * VDIM), KVRANK ** -0.5, 0.375, ((1, 4),))
    w_out = noise(key_of[9], (HEADS * VDIM, D), 0.3, 1.796875, ((0, 4),))
    tokens_b = noise(key_of[10], (TOKENS_B, D), 1.0, 6.0, ((0, 64),))
    ffn_gain = jnp.clip(1.0 + 0.18 * jax.random.normal(key_of[11], (D,), jnp.float32), 0.1, 1.9)
    route_expert = draw_route_expert(jax.random.fold_in(key_of[17], 71), 0)
    route_weight = jnp.clip(jnp.exp(math.log(1.0) - 1.609438 * jax.random.uniform(key_of[13], (TOKENS_B, TOPK), jnp.float32) ** levels(key_of[13], (TOKENS_B, TOPK), ((0, 64),), -0.2, 0.2)), 0.2, 1.0)
    w_gate = noise(key_of[14], (EXPERTS, D, FF_E), D ** -0.5, 0.125, ((0, 64), (2, 4)))
    w_up = noise(key_of[15], (EXPERTS, D, FF_E), D ** -0.5, 0.125, ((0, 64), (2, 4)))
    w_down = noise(key_of[16], (EXPERTS, FF_E, D), FF_E ** -0.5, 0.1875, ((0, 64), (1, 4)))
    return {"query_latent": query_latent, "key_latent": key_latent, "rope_key": rope_key, "query_gain": query_gain, "key_gain": key_gain, "w_query": w_query, "w_query_rope": w_query_rope, "w_key": w_key, "w_value": w_value, "w_out": w_out, "tokens_b": tokens_b, "ffn_gain": ffn_gain, "route_expert": route_expert, "route_weight": route_weight, "w_gate": w_gate, "w_up": w_up, "w_down": w_down}


epsilon = 1e-06
rotary_base = 10000.0

def rms_scale(values_in, gain):
    widened = values_in.astype(jnp.float32)
    normed = widened * lax.rsqrt(lax.optimization_barrier(jnp.mean(widened * widened, axis=-1, keepdims=True)) + epsilon)
    return (normed * gain.astype(jnp.float32)).astype(jnp.bfloat16)

def rotary_tables(positions):
    half_width = ROPE // 2
    inverse = rotary_base ** (-jnp.arange(0, half_width, 2, dtype=jnp.float32) / half_width)
    grid_row = (positions // GRID_W).astype(jnp.float32)
    grid_col = (positions % GRID_W).astype(jnp.float32)
    angle = jnp.concatenate([grid_row[:, None] * inverse, grid_col[:, None] * inverse], axis=-1)
    return (jnp.cos(angle), jnp.sin(angle))

def rotate(values_in, cosine, sine):
    even_part = values_in[..., 0::2]
    odd_part = values_in[..., 1::2]
    turned = jnp.stack([even_part * cosine - odd_part * sine, even_part * sine + odd_part * cosine], axis=-1)
    return turned.reshape(values_in.shape)

def mixer_half(query_latent, key_latent, rope_key, query_gain, key_gain, w_query, w_query_rope, w_key, w_value, w_out):
    seq_len = query_latent.shape[0]
    positions = jnp.arange(seq_len, dtype=jnp.int32)
    cosine, sine = rotary_tables(positions)
    query_normed = rms_scale(query_latent, query_gain)
    query_nope = jnp.dot(query_normed, w_query, preferred_element_type=jnp.float32).astype(jnp.bfloat16)
    query_nope = query_nope.reshape(seq_len, HEADS, NOPE)
    query_rot = jnp.dot(query_normed, w_query_rope, preferred_element_type=jnp.float32).reshape(seq_len, HEADS, ROPE)
    query_rot = rotate(query_rot, cosine[:, None, :], sine[:, None, :]).astype(jnp.bfloat16)
    key_normed = rms_scale(key_latent, key_gain)
    key_nope = jnp.dot(key_normed, w_key, preferred_element_type=jnp.float32).astype(jnp.bfloat16)
    key_nope = key_nope.reshape(seq_len, HEADS, NOPE)
    value_rows = jnp.dot(key_normed, w_value, preferred_element_type=jnp.float32).astype(jnp.bfloat16)
    value_rows = value_rows.reshape(seq_len, HEADS, VDIM)
    key_rot = rotate(rope_key.astype(jnp.float32), cosine, sine).astype(jnp.bfloat16)
    score_scale = (NOPE + ROPE) ** (-0.5)
    block_rows = math.gcd(seq_len, 512)

    def one_head(operands):
        head_query, head_rot, head_key, head_value = operands

        def one_block(block_operands):
            block_query, block_rot = block_operands
            scores = jnp.dot(block_query, head_key.T, preferred_element_type=jnp.float32)
            scores = (scores + jnp.dot(block_rot, key_rot.T, preferred_element_type=jnp.float32)) * score_scale
            row_max = lax.optimization_barrier(jnp.max(scores, axis=-1, keepdims=True))
            weights = jnp.exp(scores - row_max)
            totals = lax.optimization_barrier(jnp.sum(weights, axis=-1, keepdims=True))
            mixed = jnp.dot(weights.astype(jnp.bfloat16), head_value, preferred_element_type=jnp.float32)
            return (mixed / totals).astype(jnp.bfloat16)
        blocks = lax.map(one_block, (head_query.reshape(seq_len // block_rows, block_rows, NOPE), head_rot.reshape(seq_len // block_rows, block_rows, ROPE)))
        return blocks.reshape(seq_len, VDIM)
    heads_out = lax.map(one_head, (jnp.moveaxis(query_nope, 1, 0), jnp.moveaxis(query_rot, 1, 0), jnp.moveaxis(key_nope, 1, 0), jnp.moveaxis(value_rows, 1, 0)))
    heads_flat = jnp.moveaxis(heads_out, 0, 1).reshape(seq_len, HEADS * VDIM)
    group_cols = HEADS * VDIM // N_TP
    summed = jnp.zeros((seq_len, D), jnp.float32)
    for group_index in range(N_TP):
        lower = group_index * group_cols
        piece_sum = jnp.dot(heads_flat[:, lower:lower + group_cols], w_out[lower:lower + group_cols], preferred_element_type=jnp.float32).astype(jnp.bfloat16)
        summed = summed + lax.optimization_barrier(piece_sum).astype(jnp.float32)
    return summed.astype(jnp.bfloat16)

def expert_half(tokens_b, ffn_gain, route_expert, route_weight, w_gate, w_up, w_down):
    all_rows = tokens_b.shape[0]
    capacity = TOPK * TOK_B // EXPERTS
    normed = rms_scale(tokens_b, ffn_gain)
    copies = route_expert.reshape(N_EP, TOK_B * TOPK)
    expert_ids = jnp.arange(EXPERTS, dtype=jnp.int32)

    def block_slots(block_copies):
        chosen = (block_copies[:, None] == expert_ids[None, :]).astype(jnp.int32)
        earlier = jnp.cumsum(chosen, axis=0) - chosen
        return lax.optimization_barrier(jnp.sum(earlier * chosen, axis=1)).astype(jnp.int32)
    slot_index = lax.map(block_slots, copies)
    block_ids = jnp.arange(N_EP, dtype=jnp.int32)[:, None]
    target = (copies * (N_EP * capacity) + block_ids * capacity + slot_index).reshape(-1).astype(jnp.int32)
    source_row = jnp.zeros((EXPERTS * N_EP * capacity,), jnp.int32).at[target].set(jnp.arange(all_rows * TOPK, dtype=jnp.int32) // TOPK)
    source_row = source_row.reshape(EXPERTS, N_EP * capacity)
    unit_cols = FF_E // N_TP

    def one_expert(operands):
        row_ids, gate_weight, up_weight, down_weight = operands
        arrived = jnp.take(normed, row_ids, axis=0)
        gate_act = jnp.dot(arrived, gate_weight, preferred_element_type=jnp.float32)
        up_act = jnp.dot(arrived, up_weight, preferred_element_type=jnp.float32)
        hidden = (jax.nn.silu(gate_act) * up_act).astype(jnp.bfloat16)
        summed = jnp.zeros((arrived.shape[0], D), jnp.float32)
        for group_index in range(N_TP):
            lower = group_index * unit_cols
            piece_sum = jnp.dot(hidden[:, lower:lower + unit_cols], down_weight[lower:lower + unit_cols], preferred_element_type=jnp.float32).astype(jnp.bfloat16)
            summed = summed + lax.optimization_barrier(piece_sum).astype(jnp.float32)
        return summed.astype(jnp.bfloat16)
    results = lax.map(one_expert, (source_row, w_gate, w_up, w_down)).reshape(EXPERTS * N_EP * capacity, D)
    picked = jnp.take(results, target, axis=0).reshape(all_rows, TOPK, D)
    combined = lax.optimization_barrier(jnp.sum(picked.astype(jnp.float32) * route_weight[:, :, None], axis=1))
    return combined.astype(jnp.bfloat16)

def reference(query_latent, key_latent, rope_key, query_gain, key_gain, w_query, w_query_rope, w_key, w_value, w_out, tokens_b, ffn_gain, route_expert, route_weight, w_gate, w_up, w_down):
    mixer_out = mixer_half(query_latent, key_latent, rope_key, query_gain, key_gain, w_query, w_query_rope, w_key, w_value, w_out)
    moe_out = expert_half(tokens_b, ffn_gain, route_expert, route_weight, w_gate, w_up, w_down)
    return (mixer_out, moe_out)
```

```python
import math

import jax
import jax.numpy as jnp
import numpy as np
from jax import lax
from jax.experimental import pallas as pl
from jax.experimental.pallas import tpu as pltpu
from jax.sharding import PartitionSpec as P

NOPE = 128
ROPE = 64
GRID_W = 64
epsilon = 1e-06
rotary_base = 10000.0
LOG2E = 1.4426950408889634
SCORE_SCALE = (NOPE + ROPE) ** (-0.5)

F32 = jnp.float32
BF16 = jnp.bfloat16
MESH = pl.DeviceIdType.MESH

N_EP = 64
N_TP = 4
PER_Z = 8
N_Z = 8
CAP = 16
COLS = 512
CHUNK = PER_Z * CAP
HALF = CHUNK // 2
VMEM_LIMIT = 60 * 1024 * 1024


def rotary_consts():
    inverse = np.float32(rotary_base) ** (-np.arange(0, 32, 2, dtype=np.float32) / np.float32(32))
    inverse = inverse.astype(np.float32)
    entry = np.arange(128) % ROPE
    pair = entry // 2
    row_lane = pair < 16
    freq = inverse[pair % 16]
    row_angle = (np.arange(128, dtype=np.float32)[:, None] * freq[None, :]).astype(np.float32)
    col_angle = (np.arange(64, dtype=np.float32)[:, None] * freq[None, :]).astype(np.float32)

    def both(angle, keep):
        wide = angle.astype(np.float64)
        return [np.where(keep, fn(wide), 0.0).astype(np.float32) for fn in (np.cos, np.sin)]

    row_cos, row_sin = both(row_angle, row_lane[None, :])
    col_cos, col_sin = both(col_angle, ~row_lane[None, :])
    rows = np.stack([row_cos.reshape(64, 2, 128), row_sin.reshape(64, 2, 128)], axis=1)
    rows = rows.reshape(64, 4, 128)
    cols = np.stack([col_cos, col_sin], axis=0)
    return rows, cols


def cos_sin(rows_ref, cols_ref, ep):
    rows = rows_ref[ep]
    cos = jnp.concatenate([rows[0:1] + cols_ref[0], rows[1:2] + cols_ref[0]], axis=0)
    sin = jnp.concatenate([rows[2:3] + cols_ref[1], rows[3:4] + cols_ref[1]], axis=0)
    return cos, sin


def turn(x, cos, sin):
    lane = lax.broadcasted_iota(jnp.int32, x.shape, 1)
    swapped = jnp.where(lane % 2 == 0, -pltpu.roll(x, 127, 1), pltpu.roll(x, 1, 1))
    return x * cos + swapped * sin


def rms(x, gain):
    wide = x.astype(F32)
    normed = wide * lax.rsqrt(jnp.mean(wide * wide, axis=-1, keepdims=True) + epsilon)
    return (normed * gain).astype(BF16)


def prep_kernel(
    tok_ref, gain_ref, route_ref, klat_ref, rope_ref, kgain_ref, rows_ref, cols_ref,
    out_ref, target_ref, lat_ref, normed_ref,
):
    ep = lax.axis_index("ep")
    tp = lax.axis_index("tp")
    lane0 = pl.multiple_of(tp * COLS, COLS)
    lat_ref[0:128, :] = rms(klat_ref[...], kgain_ref[...])
    cos, sin = cos_sin(rows_ref, cols_ref, ep)
    rope = rope_ref[...].astype(F32)
    rope = jnp.concatenate([rope, rope], axis=0).T
    turned = turn(rope, cos, sin)
    low = lax.broadcasted_iota(jnp.int32, (32, 128), 1) < ROPE
    left = jnp.where(low, turned[0:32], turned[32:64])
    right = jnp.where(low, turned[64:96], turned[96:128])
    lat_ref[128:160, :] = jnp.concatenate([left, right], axis=1).astype(BF16)

    @pl.loop(0, 8)
    def _(i):
        sel = pl.ds(pl.multiple_of(i * 64, 64), 64)
        wide = tok_ref[sel, :].astype(F32)
        scale = lax.rsqrt(jnp.mean(wide * wide, axis=-1, keepdims=True) + epsilon)
        part = tok_ref[sel, pl.ds(lane0, COLS)].astype(F32)
        normed_ref[sel, :] = (part * scale * gain_ref[:, pl.ds(lane0, COLS)]).astype(BF16)

    route = route_ref[...]
    first = route[0:1, :]
    second = route[1:2, :]
    ids = lax.broadcasted_iota(jnp.int32, (N_EP, 512), 0)
    hit0 = (ids == first).astype(F32)
    hit1 = (ids == second).astype(F32)
    before = lax.broadcasted_iota(jnp.int32, (512, 512), 0) < lax.broadcasted_iota(
        jnp.int32, (512, 512), 1
    )
    earlier = jnp.dot((hit0 + hit1).astype(BF16), before.astype(BF16), preferred_element_type=F32)
    slot0 = jnp.sum(hit0 * earlier, axis=0, keepdims=True).astype(jnp.int32)
    slot1 = jnp.sum(hit1 * earlier, axis=0, keepdims=True).astype(jnp.int32)
    target0 = first * CAP + slot0
    target1 = second * CAP + slot1
    target_ref[0:1, :] = target0
    target_ref[1:2, :] = target1

    @pl.loop(0, 4)
    def _(i):
        base = i * 256
        ids = lax.broadcasted_iota(jnp.int32, (256, 512), 0) + base
        pick = ((ids == target0) | (ids == target1)).astype(BF16)
        rows = jnp.dot(pick, normed_ref[...], preferred_element_type=F32).astype(BF16)
        out_ref[pl.ds(i * CAP, CAP)] = rows.reshape(CAP, CAP, COLS)


def chunk_offset(c):
    return (c % 2) * (4 + c // 2) + (1 - c % 2) * ((4 - c // 2) % 4)


def remote(src, dst, send, recv, where):
    return pltpu.make_async_remote_copy(
        src_ref=src, dst_ref=dst, send_sem=send, recv_sem=recv, device_id=where, device_id_type=MESH
    )


def expert_kernel(
    out_ref, wg_hbm, wu_hbm, wd_hbm, ret_ref,
    wg, wu, wd, arr, part, rs1p, rs1m, rdp, rdm, sp, sm, rsp, rsm, res, hid,
    wsem, send, ra2a, ry0p, ry0m, rfwp, rfwm, r1p, r1m, r2p, r2m, r3p, r3m, rret,
):
    ep = lax.axis_index("ep")
    tp = lax.axis_index("tp")
    z = ep // PER_Z
    xc = ep % PER_Z
    up = (tp + 1) % N_TP
    down = (tp + N_TP - 1) % N_TP
    across = (tp + 2) % N_TP

    barrier = pltpu.get_barrier_semaphore()

    @pl.loop(1, N_EP)
    def _(i):
        pl.semaphore_signal(
            barrier, inc=1, device_id={"ep": (ep + i) % N_EP}, device_id_type=MESH
        )

    pl.semaphore_signal(barrier, inc=1, device_id={"tp": up}, device_id_type=MESH)
    pl.semaphore_signal(barrier, inc=1, device_id={"tp": down}, device_id_type=MESH)
    loads = [
        pltpu.make_async_copy(src, dst, wsem.at[i])
        for i, (src, dst) in enumerate(((wg_hbm, wg), (wu_hbm, wu), (wd_hbm, wd)))
    ]
    for load in loads:
        load.start()
    arr[tp, pl.ds(ep, 1)] = out_ref[pl.ds(ep, 1)]
    pl.semaphore_wait(barrier, N_EP - 1 + 2)

    @pl.loop(0, N_Z)
    def _(c):
        far = ((z + chunk_offset(c)) % N_Z) * PER_Z

        def put(other):
            remote(
                out_ref.at[other], arr.at[tp, ep], send.at[0], ra2a.at[c], {"ep": other}
            ).start()

        @pl.when(c != 0)
        def _():
            put(far + xc)

        @pl.loop(1, PER_Z)
        def _(j):
            put(far + (xc + j) % PER_Z)

    for load in loads:
        load.wait()

    def y_copy(src, dst, send_at, recv, where):
        return remote(src, dst, send.at[send_at], recv, {"tp": where})

    def plane(c):
        return ((z + N_Z - chunk_offset(c)) % N_Z) * PER_Z

    def stage0(c):
        at = plane(c)
        whole = arr.at[tp, pl.ds(at, PER_Z)]
        less = arr.at[tp, pl.ds(0, PER_Z - 1)]

        @pl.when(c == 0)
        def _():
            remote(less, less, send.at[0], ra2a.at[c], {"tp": up}).wait_recv()

        @pl.when(c != 0)
        def _():
            remote(whole, whole, send.at[0], ra2a.at[c], {"tp": up}).wait_recv()

        y_copy(whole, whole, 1, ry0p.at[c], up).start()
        y_copy(whole, whole, 2, ry0m.at[c], down).start()

    def stage1(c):
        at = plane(c)
        below = arr.at[down, pl.ds(at, PER_Z)]
        above = arr.at[up, pl.ds(at, PER_Z)]
        y_copy(below, below, 1, ry0p.at[c], up).wait_recv()
        half = arr.at[down, pl.ds(at, PER_Z // 2)]
        y_copy(half, half, 3, rfwp.at[c], up).start()
        y_copy(above, above, 2, ry0m.at[c], down).wait_recv()
        half = arr.at[up, pl.ds(at + PER_Z // 2, PER_Z // 2)]
        y_copy(half, half, 4, rfwm.at[c], down).start()

    def stage2(c):
        at = plane(c)
        half = arr.at[across, pl.ds(at, PER_Z // 2)]
        y_copy(half, half, 3, rfwp.at[c], up).wait_recv()
        half = arr.at[across, pl.ds(at + PER_Z // 2, PER_Z // 2)]
        y_copy(half, half, 4, rfwm.at[c], down).wait_recv()
        gate = jnp.zeros((CHUNK, 256), F32)
        upper = jnp.zeros((CHUNK, 256), F32)
        for q in range(N_TP):
            rows = arr[q, pl.ds(at, PER_Z)].reshape(CHUNK, COLS)
            gate += jnp.dot(rows, wg[q * COLS : (q + 1) * COLS, :], preferred_element_type=F32)
            upper += jnp.dot(rows, wu[q * COLS : (q + 1) * COLS, :], preferred_element_type=F32)
        hid[...] = (gate / (1.0 + jnp.exp(-gate)) * upper).astype(BF16)
        for q in range(N_TP):
            part[c, q] = jnp.dot(
                hid[...], wd[:, q * COLS : (q + 1) * COLS], preferred_element_type=F32
            ).astype(BF16)
        y_copy(part.at[c, across, pl.ds(0, HALF)], rs1p.at[c], 5, r1p.at[c], up).start()
        y_copy(part.at[c, across, pl.ds(HALF, HALF)], rs1m.at[c], 6, r1m.at[c], down).start()
        y_copy(part.at[c, up, pl.ds(HALF, HALF)], rdp.at[c], 7, r2p.at[c], up).start()
        y_copy(part.at[c, down, pl.ds(0, HALF)], rdm.at[c], 8, r2m.at[c], down).start()

    def stage3(c):
        y_copy(rs1p.at[c], rs1p.at[c], 5, r1p.at[c], up).wait_recv()
        sp[c] = (rs1p[c].astype(F32) + part[c, up, 0:HALF].astype(F32)).astype(BF16)
        y_copy(sp.at[c], rsp.at[c], 9, r3p.at[c], up).start()
        y_copy(rs1m.at[c], rs1m.at[c], 6, r1m.at[c], down).wait_recv()
        sm[c] = (rs1m[c].astype(F32) + part[c, down, HALF:CHUNK].astype(F32)).astype(BF16)
        y_copy(sm.at[c], rsm.at[c], 10, r3m.at[c], down).start()

    def stage4(c):
        at = plane(c)
        y_copy(rdp.at[c], rdp.at[c], 7, r2p.at[c], up).wait_recv()
        y_copy(rdm.at[c], rdm.at[c], 8, r2m.at[c], down).wait_recv()
        y_copy(rsp.at[c], rsp.at[c], 9, r3p.at[c], up).wait_recv()
        y_copy(rsm.at[c], rsm.at[c], 10, r3m.at[c], down).wait_recv()
        top = part[c, tp, 0:HALF].astype(F32) + rsp[c].astype(F32) + rdm[c].astype(F32)
        low = part[c, tp, HALF:CHUNK].astype(F32) + rdp[c].astype(F32) + rsm[c].astype(F32)
        res[c, 0 : PER_Z // 2] = top.astype(BF16).reshape(PER_Z // 2, CAP, COLS)
        res[c, PER_Z // 2 : PER_Z] = low.astype(BF16).reshape(PER_Z // 2, CAP, COLS)

        def put(j):
            remote(
                res.at[c, j], ret_ref.at[ep], send.at[11], rret.at[c], {"ep": at + j}
            ).start()

        @pl.when(c != 0)
        def _():
            put(xc)

        @pl.when(c == 0)
        def _():
            ret_ref[pl.ds(ep, 1)] = res[c, pl.ds(xc, 1)]

        @pl.loop(1, PER_Z)
        def _(j):
            put((xc + j) % PER_Z)

    stages = (stage0, stage1, stage2, stage3, stage4)

    @pl.loop(0, N_Z + len(stages) - 1)
    def _(i):
        for lag, stage in enumerate(stages):

            @pl.when((i >= lag) & (i < N_Z + lag))
            def _(stage=stage, lag=lag):
                stage(i - lag)

    @pl.loop(0, N_Z)
    def _(c):
        far = ((z + chunk_offset(c)) % N_Z) * PER_Z
        whole = ret_ref.at[pl.ds(far, PER_Z)]
        less = ret_ref.at[pl.ds(0, PER_Z - 1)]

        @pl.when(c == 0)
        def _():
            remote(less, less, send.at[11], rret.at[c], {"tp": up}).wait_recv()

        @pl.when(c != 0)
        def _():
            remote(whole, whole, send.at[11], rret.at[c], {"tp": up}).wait_recv()

    def sent(ref, which):
        remote(ref, ref, send.at[which], ra2a.at[0], {"tp": up}).wait_send()

    sent(out_ref.at[pl.ds(0, N_EP - 1)], 0)
    sent(arr.at[0], 1)
    sent(arr.at[0], 2)
    sent(arr.at[0, pl.ds(0, N_EP // 2)], 3)
    sent(arr.at[0, pl.ds(0, N_EP // 2)], 4)
    for which in range(5, 11):
        sent(rs1p, which)
    sent(out_ref.at[pl.ds(0, N_EP - 1)], 11)


def combine_kernel(target_ref, weight_ref, ret_ref, out_ref):
    pad = jnp.zeros((124, 512), F32)
    both = jnp.concatenate([target_ref[...].astype(F32), weight_ref[...], pad], axis=0)
    turned = both.T
    for i in range(4):
        rows = turned[i * 128 : (i + 1) * 128]
        ids = lax.broadcasted_iota(jnp.int32, (128, 1024), 1)
        total = jnp.zeros((128, COLS), F32)
        for c in range(2):
            pick = (ids == rows[:, c : c + 1].astype(jnp.int32)).astype(BF16)
            got = jnp.dot(pick, ret_ref[...], preferred_element_type=F32)
            total = total + got * rows[:, 2 + c : 3 + c]
        out_ref[i * 128 : (i + 1) * 128, :] = total.astype(BF16)


def mixer_kernel(
    qlat_ref, qgain_ref, wq_ref, wqr_ref, wk_ref, wv_ref, wo_ref, rows_ref, cols_ref, lat_ref,
    out_ref, qrot, top, total, acc, mix, got, send, recv,
):
    ep = lax.axis_index("ep")
    tp = lax.axis_index("tp")
    barrier = pltpu.get_barrier_semaphore()
    for i in range(1, N_TP):
        pl.semaphore_signal(
            barrier, inc=1, device_id={"tp": (tp + i) % N_TP}, device_id_type=MESH
        )
    qn = rms(qlat_ref[...], qgain_ref[...])
    nope = jnp.dot(qn, wq_ref[...], preferred_element_type=F32).astype(BF16)
    absorbed = [
        lax.dot_general(
            nope[:, h * 128 : (h + 1) * 128],
            wk_ref[:, h * 128 : (h + 1) * 128],
            (((1,), (1,)), ((), ())),
            preferred_element_type=F32,
        ).astype(BF16)
        for h in range(2)
    ]
    query = jnp.concatenate(absorbed, axis=0)
    cos, sin = cos_sin(rows_ref, cols_ref, ep)
    rot = turn(jnp.dot(qn, wqr_ref[...], preferred_element_type=F32), cos, sin)
    low = lax.broadcasted_iota(jnp.int32, (128, 128), 1) < ROPE
    rolled = pltpu.roll(rot, ROPE, 1)
    first = jnp.concatenate([jnp.where(low, rot, 0.0), jnp.where(low, rolled, 0.0)], axis=0)
    second = jnp.concatenate([jnp.where(low, 0.0, rolled), jnp.where(low, 0.0, rot)], axis=0)
    first = first.astype(BF16)
    second = second.astype(BF16)
    none = jnp.zeros((256, 128), BF16)
    for g, pair in enumerate(((first, none), (second, none), (none, first), (none, second))):
        qrot[g] = jnp.concatenate(pair, axis=1)
    top[...] = jnp.full((256, 1), -1e30, F32)
    total[...] = jnp.zeros((256, 1), F32)
    acc[...] = jnp.zeros((256, 256), F32)

    @pl.loop(0, 8)
    def _(i):
        g = i // 2
        blocks = pl.ds((i % 2) * 32, 32)
        keys = lat_ref[blocks, pl.ds(pl.multiple_of(g * 32, 32), 32), :].reshape(1024, 256)
        turned = lat_ref[blocks, 128:160, :].reshape(1024, 256)
        dims = (((1,), (1,)), ((), ()))
        scores = lax.dot_general(query, keys, dims, preferred_element_type=F32)
        scores += lax.dot_general(qrot[g], turned, dims, preferred_element_type=F32)
        scores = scores * (SCORE_SCALE * LOG2E)
        new_top = jnp.maximum(top[...], jnp.max(scores, axis=1, keepdims=True))
        fade = jnp.exp2(top[...] - new_top)
        weights = jnp.exp2(scores - new_top)
        total[...] = total[...] * fade + jnp.sum(weights, axis=1, keepdims=True)
        acc[...] = acc[...] * fade + jnp.dot(
            weights.astype(BF16), keys, preferred_element_type=F32
        )
        top[...] = new_top

    mean = (acc[...] / total[...]).astype(BF16)
    heads = [
        jnp.dot(
            mean[h * 128 : (h + 1) * 128],
            wv_ref[:, h * 128 : (h + 1) * 128],
            preferred_element_type=F32,
        ).astype(BF16)
        for h in range(2)
    ]
    heads = jnp.concatenate(heads, axis=1)
    for q in range(4):
        cols = slice(q * 512, (q + 1) * 512)
        mix[:, :, cols] = (
            jnp.dot(heads, wo_ref[:, cols], preferred_element_type=F32)
            .astype(BF16)
            .reshape(N_TP, 32, 512)
        )
    pl.semaphore_wait(barrier, N_TP - 1)
    copies = []
    for i in range(1, N_TP):
        other = (tp + i) % N_TP
        copies.append(remote(mix.at[other], got.at[i], send.at[i], recv.at[i], {"tp": other}))
        copies[-1].start()
    sums = mix[tp].astype(F32)
    for i in range(1, N_TP):
        copies[i - 1].wait()
        sums = sums + got[i].astype(F32)
    out_ref[...] = sums.astype(BF16)


VM = pl.BlockSpec(memory_space=pltpu.VMEM)
ANY = pl.BlockSpec(memory_space=pl.ANY)


def struct(shape, dtype=BF16):
    return jax.ShapeDtypeStruct(shape, dtype)


def body(
    query_latent, key_latent, rope_key, query_gain, key_gain, w_query, w_query_rope, w_key,
    w_value, w_out, tokens_b, ffn_gain, route_expert, route_weight, w_gate, w_up, w_down,
):
    rows_np, cols_np = rotary_consts()
    rows = jnp.asarray(rows_np)
    cols = jnp.asarray(cols_np)
    dma = pltpu.SemaphoreType.DMA

    outgoing, target, lat = pl.pallas_call(
        prep_kernel,
        out_shape=(
            struct((N_EP, CAP, COLS)),
            struct((2, 512), jnp.int32),
            struct((160, 256)),
        ),
        in_specs=[VM] * 8,
        out_specs=(VM, VM, VM),
        scratch_shapes=[pltpu.VMEM((512, COLS), BF16)],
        compiler_params=pltpu.CompilerParams(vmem_limit_bytes=VMEM_LIMIT),
        name="prep",
    )(
        tokens_b, ffn_gain.reshape(1, -1), route_expert.T, key_latent, rope_key.T,
        key_gain.reshape(1, -1), rows, cols,
    )
    gathered = lax.all_gather(lat, "ep", axis=0, tiled=True).reshape(N_EP, 160, 256)

    half = (N_Z, HALF, COLS)
    returned = pl.pallas_call(
        expert_kernel,
        out_shape=struct((N_EP, CAP, COLS)),
        in_specs=[VM, ANY, ANY, ANY],
        out_specs=VM,
        scratch_shapes=[
            pltpu.VMEM((2048, 256), BF16),
            pltpu.VMEM((2048, 256), BF16),
            pltpu.VMEM((256, 2048), BF16),
            pltpu.VMEM((N_TP, N_EP, CAP, COLS), BF16),
            pltpu.VMEM((N_Z, N_TP, CHUNK, COLS), BF16),
        ]
        + [pltpu.VMEM(half, BF16)] * 8
        + [
            pltpu.VMEM((N_Z, PER_Z, CAP, COLS), BF16),
            pltpu.VMEM((CHUNK, 256), BF16),
            dma((3,)),
            dma((12,)),
        ]
        + [dma((N_Z,))] * 12,
        compiler_params=pltpu.CompilerParams(
            collective_id=0, has_side_effects=True, vmem_limit_bytes=VMEM_LIMIT
        ),
        cost_estimate=pl.CostEstimate(flops=80_000_000_000, bytes_accessed=8_000_000, transcendentals=0),
        name="experts",
    )(outgoing, w_gate[0], w_up[0], w_down[0])

    moe_out = pl.pallas_call(
        combine_kernel,
        out_shape=struct((512, COLS)),
        in_specs=[VM] * 3,
        out_specs=VM,
        compiler_params=pltpu.CompilerParams(vmem_limit_bytes=VMEM_LIMIT),
        name="combine",
    )(target, route_weight.T, returned.reshape(N_EP * CAP, COLS))

    mixer_out = pl.pallas_call(
        mixer_kernel,
        out_shape=struct((32, 2048)),
        in_specs=[VM] * 10,
        out_specs=VM,
        scratch_shapes=[
            pltpu.VMEM((4, 256, 256), BF16),
            pltpu.VMEM((256, 1), F32),
            pltpu.VMEM((256, 1), F32),
            pltpu.VMEM((256, 256), F32),
            pltpu.VMEM((N_TP, 32, 2048), BF16),
            pltpu.VMEM((N_TP, 32, 2048), BF16),
            dma((N_TP,)),
            dma((N_TP,)),
        ],
        compiler_params=pltpu.CompilerParams(
            collective_id=1, has_side_effects=True, vmem_limit_bytes=VMEM_LIMIT
        ),
        cost_estimate=pl.CostEstimate(flops=8_000_000_000, bytes_accessed=8_000_000, transcendentals=0),
        name="mixer",
    )(
        query_latent, query_gain.reshape(1, -1), w_query, w_query_rope, w_key, w_value, w_out,
        rows, cols, gathered,
    )
    return (mixer_out, moe_out)


def solution(mesh):
    in_specs = (
        P("ep", None),
        P("ep", None),
        P("ep", None),
        P(),
        P(),
        P(None, "tp"),
        P(None, "tp"),
        P(None, "tp"),
        P(None, "tp"),
        P("tp", None),
        P("ep", None),
        P(),
        P("ep", None),
        P("ep", None),
        P("ep", None, "tp"),
        P("ep", None, "tp"),
        P("ep", "tp", None),
    )
    out_specs = (P(("ep", "tp"), None), P("ep", "tp"))
    return jax.shard_map(body, mesh=mesh, in_specs=in_specs, out_specs=out_specs, check_vma=False)
```

```python
import math

import jax
import jax.numpy as jnp
import numpy as np
from jax import lax
from jax.experimental import pallas as pl
from jax.experimental.pallas import tpu as pltpu
from jax.sharding import PartitionSpec as P

NOPE = 128
ROPE = 64
GRID_W = 64
epsilon = 1e-06
rotary_base = 10000.0
LOG2E = 1.4426950408889634
SCORE_SCALE = (NOPE + ROPE) ** (-0.5)

F32 = jnp.float32
BF16 = jnp.bfloat16
MESH = pl.DeviceIdType.MESH

N_EP = 64
N_TP = 4
PER_Z = 8
N_Z = 8
CAP = 16
COLS = 512
CHUNK = PER_Z * CAP
HALF = CHUNK // 2
VMEM_LIMIT = 60 * 1024 * 1024


def rotary_consts():
    inverse = np.float32(rotary_base) ** (-np.arange(0, 32, 2, dtype=np.float32) / np.float32(32))
    inverse = inverse.astype(np.float32)
    entry = np.arange(128) % ROPE
    pair = entry // 2
    row_lane = pair < 16
    freq = inverse[pair % 16]
    row_angle = (np.arange(128, dtype=np.float32)[:, None] * freq[None, :]).astype(np.float32)
    col_angle = (np.arange(64, dtype=np.float32)[:, None] * freq[None, :]).astype(np.float32)

    def both(angle, keep):
        wide = angle.astype(np.float64)
        return [np.where(keep, fn(wide), 0.0).astype(np.float32) for fn in (np.cos, np.sin)]

    row_cos, row_sin = both(row_angle, row_lane[None, :])
    col_cos, col_sin = both(col_angle, ~row_lane[None, :])
    rows = np.stack([row_cos.reshape(64, 2, 128), row_sin.reshape(64, 2, 128)], axis=1)
    rows = rows.reshape(64, 4, 128)
    cols = np.stack([col_cos, col_sin], axis=0)
    return rows, cols


def cos_sin(rows_ref, cols_ref, ep):
    rows = rows_ref[ep]
    cos = jnp.concatenate([rows[0:1] + cols_ref[0], rows[1:2] + cols_ref[0]], axis=0)
    sin = jnp.concatenate([rows[2:3] + cols_ref[1], rows[3:4] + cols_ref[1]], axis=0)
    return cos, sin


def turn(x, cos, sin):
    lane = lax.broadcasted_iota(jnp.int32, x.shape, 1)
    swapped = jnp.where(lane % 2 == 0, -pltpu.roll(x, 127, 1), pltpu.roll(x, 1, 1))
    return x * cos + swapped * sin


def rms(x, gain):
    wide = x.astype(F32)
    normed = wide * lax.rsqrt(jnp.mean(wide * wide, axis=-1, keepdims=True) + epsilon)
    return (normed * gain).astype(BF16)


NT = (((1,), (1,)), ((), ()))


def chunk_offset(c):
    return (c % 2) * (4 + c // 2) + (1 - c % 2) * ((4 - c // 2) % 4)


def remote(src, dst, send, recv, where):
    return pltpu.make_async_remote_copy(
        src_ref=src, dst_ref=dst, send_sem=send, recv_sem=recv, device_id=where, device_id_type=MESH
    )


def main_kernel(
    gain_ref, route_ref, klat_ref, rope_ref, kgain_ref, qlat_ref, qgain_ref, rows_ref, cols_ref,
    tok_hbm, wg_hbm, wu_hbm, wd_hbm, wq_hbm, wqr_hbm, wk_hbm, wv_hbm, wo_hbm,
    ret_ref, target_ref, mixed_ref,
    tok, wg, wu, wq, wqr, wk, wv, wo, wdq, relay_p, relay_m,
    normed, outg, arr, hid, res, lat, query, qrot, top, total, acc, mix, got,
    wsem, send, rwd, rmix, ra2a, ry0p, ry0m, rfwp, rfwm, rh0p, rh0m, rhfp, rhfm, rret, rlz, rlx, rld,
):
    ep = lax.axis_index("ep")
    tp = lax.axis_index("tp")
    z = ep // PER_Z
    xc = ep % PER_Z
    x = xc // 2
    core = xc % 2
    up = (tp + 1) % N_TP
    down = (tp + N_TP - 1) % N_TP
    across = (tp + 2) % N_TP

    barrier = pltpu.get_barrier_semaphore()

    @pl.loop(1, N_EP)
    def _(i):
        pl.semaphore_signal(
            barrier, inc=1, device_id={"ep": (ep + i) % N_EP}, device_id_type=MESH
        )

    for other in (up, down, across):
        pl.semaphore_signal(barrier, inc=1, device_id={"tp": other}, device_id_type=MESH)

    def columns(which):
        return pl.ds(pl.multiple_of(which * COLS, COLS), COLS)

    pairs = (
        (tok_hbm, tok), (wd_hbm.at[:, columns(tp)], wdq.at[tp]), (wg_hbm, wg), (wu_hbm, wu),
        (wq_hbm, wq), (wqr_hbm, wqr), (wk_hbm, wk), (wv_hbm, wv), (wo_hbm, wo),
    )
    loads = [pltpu.make_async_copy(src, dst, wsem.at[i]) for i, (src, dst) in enumerate(pairs)]
    for load in loads:
        load.start()

    cos, sin = cos_sin(rows_ref, cols_ref, ep)
    lat[core, z, x, 0:128, :] = rms(klat_ref[...], kgain_ref[...])
    rope = rope_ref[...].astype(F32)
    rope = jnp.concatenate([rope, rope], axis=0).T
    turned = turn(rope, cos, sin)
    low = lax.broadcasted_iota(jnp.int32, (32, 128), 1) < ROPE
    left = jnp.where(low, turned[0:32], turned[32:64])
    right = jnp.where(low, turned[64:96], turned[96:128])
    lat[core, z, x, 128:160, :] = jnp.concatenate([left, right], axis=1).astype(BF16)

    route = route_ref[...]
    first = route[0:1, :]
    second = route[1:2, :]
    ids = lax.broadcasted_iota(jnp.int32, (N_EP, 512), 0)
    hit0 = (ids == first).astype(F32)
    hit1 = (ids == second).astype(F32)
    before = lax.broadcasted_iota(jnp.int32, (512, 512), 0) < lax.broadcasted_iota(
        jnp.int32, (512, 512), 1
    )
    earlier = jnp.dot((hit0 + hit1).astype(BF16), before.astype(BF16), preferred_element_type=F32)
    slot0 = jnp.sum(hit0 * earlier, axis=0, keepdims=True).astype(jnp.int32)
    slot1 = jnp.sum(hit1 * earlier, axis=0, keepdims=True).astype(jnp.int32)
    target_ref[0:1, :] = first * CAP + slot0
    target_ref[1:2, :] = second * CAP + slot1

    loads[0].wait()

    @pl.loop(0, 8)
    def _(i):
        sel = pl.ds(pl.multiple_of(i * 64, 64), 64)
        wide = tok[sel, :].astype(F32)
        scale = lax.rsqrt(jnp.mean(wide * wide, axis=-1, keepdims=True) + epsilon)
        part = tok[sel, columns(tp)].astype(F32)
        normed[sel, :] = (part * scale * gain_ref[:, columns(tp)]).astype(BF16)

    @pl.loop(0, 4)
    def _(i):
        ids = lax.broadcasted_iota(jnp.int32, (256, 512), 0) + i * 256
        pick = ((ids == target_ref[0:1, :]) | (ids == target_ref[1:2, :])).astype(BF16)
        rows = jnp.dot(pick, normed[...], preferred_element_type=F32).astype(BF16)
        outg[pl.ds(i * CAP, CAP)] = rows.reshape(CAP, CAP, COLS)

    arr[tp, pl.ds(ep, 1)] = outg[pl.ds(ep, 1)]
    pl.semaphore_wait(barrier, N_EP - 1 + 3)

    def y_copy(src, dst, send_at, recv, where):
        return remote(src, dst, send.at[send_at], recv, {"tp": where})

    y_copy(wd_hbm.at[:, columns(up)], wdq.at[tp], 0, rwd.at[0], up).start()
    y_copy(wd_hbm.at[:, columns(down)], wdq.at[tp], 1, rwd.at[1], down).start()
    y_copy(wd_hbm.at[pl.ds(0, 128), columns(across)], relay_p, 2, rwd.at[2], up).start()
    y_copy(wd_hbm.at[pl.ds(128, 128), columns(across)], relay_m, 3, rwd.at[3], down).start()

    @pl.loop(0, N_Z)
    def _(c):
        zd = (z + chunk_offset(c)) % N_Z
        far = zd * PER_Z

        def put(other):
            remote(outg.at[other], arr.at[tp, ep], send.at[6], ra2a.at[c], {"ep": other}).start()

        @pl.when(c != 0)
        def _():
            put(far + xc)

        @pl.loop(1, PER_Z)
        def _(j):
            put(far + (xc + j) % PER_Z)

        @pl.when(c != 0)
        def _():
            mine = lat.at[core, z, x]
            remote(mine, mine, send.at[7], rlz.at[c], {"ep": far + xc}).start()

    for load in loads[1:]:
        load.wait()

    qn = rms(qlat_ref[...], qgain_ref[...])
    nope = jnp.dot(qn, wq[...], preferred_element_type=F32).astype(BF16)
    for h in range(2):
        sel = slice(h * 128, (h + 1) * 128)
        query[sel, :] = lax.dot_general(
            nope[:, sel], wk[:, sel], NT, preferred_element_type=F32
        ).astype(BF16)
    rot = turn(jnp.dot(qn, wqr[...], preferred_element_type=F32), cos, sin)
    low = lax.broadcasted_iota(jnp.int32, (128, 128), 1) < ROPE
    rolled = pltpu.roll(rot, ROPE, 1)
    near = jnp.concatenate([jnp.where(low, rot, 0.0), jnp.where(low, rolled, 0.0)], axis=0)
    far = jnp.concatenate([jnp.where(low, 0.0, rolled), jnp.where(low, 0.0, rot)], axis=0)
    near = near.astype(BF16)
    far = far.astype(BF16)
    none = jnp.zeros((256, 128), BF16)
    for g, pair in enumerate(((near, none), (far, none), (none, near), (none, far))):
        qrot[g] = jnp.concatenate(pair, axis=1)
    top[...] = jnp.full((256, 1), -1e30, F32)
    total[...] = jnp.zeros((256, 1), F32)
    acc[...] = jnp.zeros((256, 256), F32)

    y_copy(relay_p, relay_p, 2, rwd.at[2], up).wait_recv()
    y_copy(relay_p, wdq.at[down, pl.ds(0, 128)], 4, rwd.at[4], up).start()
    y_copy(relay_m, relay_m, 3, rwd.at[3], down).wait_recv()
    y_copy(relay_m, wdq.at[up, pl.ds(128, 128)], 5, rwd.at[5], down).start()

    def plane(c):
        return (z + N_Z - chunk_offset(c)) % N_Z

    def tokens_in(c):
        at = plane(c) * PER_Z
        whole = arr.at[tp, pl.ds(at, PER_Z)]
        less = arr.at[tp, pl.ds(0, PER_Z - 1)]

        @pl.when(c == 0)
        def _():
            remote(less, less, send.at[6], ra2a.at[c], {"tp": up}).wait_recv()

        @pl.when(c != 0)
        def _():
            remote(whole, whole, send.at[6], ra2a.at[c], {"tp": up}).wait_recv()

        y_copy(whole, whole, 8, ry0p.at[c], up).start()
        y_copy(whole, whole, 9, ry0m.at[c], down).start()

    def tokens_on(c):
        at = plane(c) * PER_Z
        below = arr.at[down, pl.ds(at, PER_Z)]
        above = arr.at[up, pl.ds(at, PER_Z)]
        y_copy(below, below, 8, ry0p.at[c], up).wait_recv()
        half = arr.at[down, pl.ds(at, PER_Z // 2)]
        y_copy(half, half, 10, rfwp.at[c], up).start()
        y_copy(above, above, 9, ry0m.at[c], down).wait_recv()
        half = arr.at[up, pl.ds(at + PER_Z // 2, PER_Z // 2)]
        y_copy(half, half, 11, rfwm.at[c], down).start()

    def hidden_units(c):
        at = plane(c) * PER_Z
        half = arr.at[across, pl.ds(at, PER_Z // 2)]
        y_copy(half, half, 10, rfwp.at[c], up).wait_recv()
        half = arr.at[across, pl.ds(at + PER_Z // 2, PER_Z // 2)]
        y_copy(half, half, 11, rfwm.at[c], down).wait_recv()
        gate = jnp.zeros((CHUNK, 256), F32)
        upper = jnp.zeros((CHUNK, 256), F32)
        for q in range(N_TP):
            rows = arr[q, pl.ds(at, PER_Z)].reshape(CHUNK, COLS)
            gate += jnp.dot(rows, wg[q * COLS : (q + 1) * COLS, :], preferred_element_type=F32)
            upper += jnp.dot(rows, wu[q * COLS : (q + 1) * COLS, :], preferred_element_type=F32)
        hid[c, tp] = (gate / (1.0 + jnp.exp(-gate)) * upper).astype(BF16)
        mine = hid.at[c, tp]
        y_copy(mine, mine, 12, rh0p.at[c], up).start()
        y_copy(mine, mine, 13, rh0m.at[c], down).start()

    def hidden_on(c):
        y_copy(hid.at[c, down], hid.at[c, down], 12, rh0p.at[c], up).wait_recv()
        half = hid.at[c, down, pl.ds(0, HALF)]
        y_copy(half, half, 14, rhfp.at[c], up).start()
        y_copy(hid.at[c, up], hid.at[c, up], 13, rh0m.at[c], down).wait_recv()
        half = hid.at[c, up, pl.ds(HALF, HALF)]
        y_copy(half, half, 15, rhfm.at[c], down).start()

    def results_out(c):
        at = plane(c) * PER_Z

        @pl.when(c == 0)
        def _():
            whole = wdq.at[0]
            half = wdq.at[0, pl.ds(0, 128)]
            y_copy(whole, whole, 0, rwd.at[0], up).wait_recv()
            y_copy(whole, whole, 1, rwd.at[1], down).wait_recv()
            y_copy(half, half, 4, rwd.at[4], up).wait_recv()
            y_copy(half, half, 5, rwd.at[5], down).wait_recv()

        half = hid.at[c, across, pl.ds(0, HALF)]
        y_copy(half, half, 14, rhfp.at[c], up).wait_recv()
        half = hid.at[c, across, pl.ds(HALF, HALF)]
        y_copy(half, half, 15, rhfm.at[c], down).wait_recv()
        sums = jnp.zeros((CHUNK, COLS), F32)
        for q in range(N_TP):
            term = jnp.dot(hid[c, q], wdq[q], preferred_element_type=F32)
            sums += term.astype(BF16).astype(F32)
        res[c] = sums.astype(BF16).reshape(PER_Z, CAP, COLS)

        def put(j):
            remote(
                res.at[c, j], ret_ref.at[ep], send.at[16], rret.at[c], {"ep": at + j}
            ).start()

        @pl.when(c != 0)
        def _():
            put(xc)

        @pl.when(c == 0)
        def _():
            ret_ref[pl.ds(ep, 1)] = res[c, pl.ds(xc, 1)]

        @pl.loop(1, PER_Z)
        def _(j):
            put((xc + j) % PER_Z)

    def latents_x(c):
        block = lat.at[core, plane(c), x]

        @pl.when(c != 0)
        def _():
            remote(block, block, send.at[7], rlz.at[c], {"tp": up}).wait_recv()

        @pl.loop(1, 4)
        def _(j):
            there = z * PER_Z + ((x + j) % 4) * 2 + core
            remote(block, block, send.at[17], rlx.at[c], {"ep": there}).start()

    def latents_core(c):
        three = lat.at[core, 0, pl.ds(0, 3)]
        remote(three, three, send.at[17], rlx.at[c], {"tp": up}).wait_recv()
        four = lat.at[core, plane(c)]
        remote(four, four, send.at[18], rld.at[c], {"ep": z * PER_Z + x * 2 + (1 - core)}).start()

    def attend(c):
        at = plane(c)
        four = lat.at[1 - core, at]
        remote(four, four, send.at[18], rld.at[c], {"tp": up}).wait_recv()
        turned = lat[:, at, :, 128:160, :].reshape(256, 256)
        keys = []
        scores = []
        for g in range(4):
            keys.append(lat[:, at, :, g * 32 : (g + 1) * 32, :].reshape(256, 256))
            s = lax.dot_general(query[...], keys[g], NT, preferred_element_type=F32)
            s += lax.dot_general(qrot[g], turned, NT, preferred_element_type=F32)
            scores.append(s * (SCORE_SCALE * LOG2E))
        peak = jnp.maximum(
            jnp.maximum(scores[0], scores[1]), jnp.maximum(scores[2], scores[3])
        )
        new_top = jnp.maximum(top[...], jnp.max(peak, axis=1, keepdims=True))
        fade = jnp.exp2(top[...] - new_top)
        weighed = acc[...] * fade
        sums = jnp.zeros((256, 256), F32)
        for g in range(4):
            weights = jnp.exp2(scores[g] - new_top)
            sums += weights
            weighed += jnp.dot(weights.astype(BF16), keys[g], preferred_element_type=F32)
        total[...] = total[...] * fade + jnp.sum(sums, axis=1, keepdims=True)
        acc[...] = weighed
        top[...] = new_top

    def mix_copy(i):
        other = (tp + i) % N_TP
        return remote(mix.at[other], got.at[i], send.at[18 + i], rmix.at[i], {"tp": other})

    def project(c):
        mean = (acc[...] / total[...]).astype(BF16)
        heads = []
        for h in range(2):
            sel = slice(h * 128, (h + 1) * 128)
            heads.append(
                jnp.dot(mean[sel], wv[:, sel], preferred_element_type=F32).astype(BF16)
            )
        heads = jnp.concatenate(heads, axis=1)
        for q in range(4):
            sel = slice(q * 512, (q + 1) * 512)
            term = jnp.dot(heads, wo[:, sel], preferred_element_type=F32)
            mix[:, :, sel] = term.astype(BF16).reshape(N_TP, 32, 512)
        for i in range(1, N_TP):
            mix_copy(i).start()

    plan = (
        (0, N_Z, tokens_in),
        (0, N_Z, latents_x),
        (1, N_Z, tokens_on),
        (1, N_Z, latents_core),
        (2, N_Z, hidden_units),
        (2, N_Z, attend),
        (3, N_Z, hidden_on),
        (4, N_Z, results_out),
        (10, 1, project),
    )

    @pl.loop(0, 12)
    def _(i):
        for lag, count, stage in plan:

            @pl.when((i >= lag) & (i < lag + count))
            def _(stage=stage, lag=lag):
                stage(i - lag)

    sums = mix[tp].astype(F32)
    for i in range(1, N_TP):
        mix_copy(i).wait()
        sums = sums + got[i].astype(F32)
    mixed_ref[...] = sums.astype(BF16)

    @pl.loop(0, N_Z)
    def _(c):
        far = ((z + chunk_offset(c)) % N_Z) * PER_Z
        whole = ret_ref.at[pl.ds(far, PER_Z)]
        less = ret_ref.at[pl.ds(0, PER_Z - 1)]

        @pl.when(c == 0)
        def _():
            remote(less, less, send.at[16], rret.at[c], {"tp": up}).wait_recv()

        @pl.when(c != 0)
        def _():
            remote(whole, whole, send.at[16], rret.at[c], {"tp": up}).wait_recv()

    def sent(ref, which):
        remote(ref, ref, send.at[which], ra2a.at[0], {"tp": up}).wait_send()

    for which in (0, 1):
        sent(wdq.at[0], which)
    for which in (2, 3, 4, 5):
        sent(relay_p, which)
    sent(outg.at[pl.ds(0, N_EP - 1)], 6)
    sent(lat.at[0, pl.ds(0, 7), 0], 7)
    for which in (8, 9):
        sent(arr.at[0], which)
    for which in (10, 11):
        sent(arr.at[0, pl.ds(0, N_EP // 2)], which)
    for which in (12, 13):
        sent(hid.at[:, 0], which)
    for which in (14, 15):
        sent(hid.at[:, 0, pl.ds(0, HALF)], which)
    sent(outg.at[pl.ds(0, N_EP - 1)], 16)
    sent(lat.at[0, :, pl.ds(0, 3)], 17)
    sent(lat.at[0], 18)


def combine_kernel(target_ref, weight_ref, ret_ref, out_ref):
    pad = jnp.zeros((124, 512), F32)
    both = jnp.concatenate([target_ref[...].astype(F32), weight_ref[...], pad], axis=0)
    turned = both.T
    for i in range(4):
        rows = turned[i * 128 : (i + 1) * 128]
        ids = lax.broadcasted_iota(jnp.int32, (128, 1024), 1)
        total = jnp.zeros((128, COLS), F32)
        for c in range(2):
            pick = (ids == rows[:, c : c + 1].astype(jnp.int32)).astype(BF16)
            got = jnp.dot(pick, ret_ref[...], preferred_element_type=F32)
            total = total + got * rows[:, 2 + c : 3 + c]
        out_ref[i * 128 : (i + 1) * 128, :] = total.astype(BF16)


VM = pl.BlockSpec(memory_space=pltpu.VMEM)
ANY = pl.BlockSpec(memory_space=pl.ANY)


def struct(shape, dtype=BF16):
    return jax.ShapeDtypeStruct(shape, dtype)


def body(
    query_latent, key_latent, rope_key, query_gain, key_gain, w_query, w_query_rope, w_key,
    w_value, w_out, tokens_b, ffn_gain, route_expert, route_weight, w_gate, w_up, w_down,
):
    rows_np, cols_np = rotary_consts()
    rows = jnp.asarray(rows_np)
    cols = jnp.asarray(cols_np)
    dma = pltpu.SemaphoreType.DMA

    returned, target, mixer_out = pl.pallas_call(
        main_kernel,
        out_shape=(
            struct((N_EP, CAP, COLS)),
            struct((2, 512), jnp.int32),
            struct((32, 2048)),
        ),
        in_specs=[VM] * 9 + [ANY] * 9,
        out_specs=(VM, VM, VM),
        scratch_shapes=[
            pltpu.VMEM(shape, dtype)
            for shape, dtype in (
                ((512, 2048), BF16),
                ((2048, 256), BF16),
                ((2048, 256), BF16),
                ((512, 256), BF16),
                ((512, 128), BF16),
                ((256, 256), BF16),
                ((256, 256), BF16),
                ((256, 2048), BF16),
                ((N_TP, 256, COLS), BF16),
                ((128, COLS), BF16),
                ((128, COLS), BF16),
                ((512, COLS), BF16),
                ((N_EP, CAP, COLS), BF16),
                ((N_TP, N_EP, CAP, COLS), BF16),
                ((N_Z, N_TP, CHUNK, 256), BF16),
                ((N_Z, PER_Z, CAP, COLS), BF16),
                ((2, N_Z, 4, 160, 256), BF16),
                ((256, 256), BF16),
                ((4, 256, 256), BF16),
                ((256, 1), F32),
                ((256, 1), F32),
                ((256, 256), F32),
                ((N_TP, 32, 2048), BF16),
                ((N_TP, 32, 2048), BF16),
            )
        ]
        + [dma((9,)), dma((22,)), dma((6,)), dma((N_TP,))]
        + [dma((N_Z,))] * 13,
        compiler_params=pltpu.CompilerParams(
            collective_id=0, has_side_effects=True, vmem_limit_bytes=VMEM_LIMIT
        ),
        name="exchange",
    )(
        ffn_gain.reshape(1, -1), route_expert.T, key_latent, rope_key.T, key_gain.reshape(1, -1),
        query_latent, query_gain.reshape(1, -1), rows, cols,
        tokens_b, w_gate[0], w_up[0], w_down[0], w_query, w_query_rope, w_key, w_value, w_out,
    )

    moe_out = pl.pallas_call(
        combine_kernel,
        out_shape=struct((512, COLS)),
        in_specs=[VM] * 3,
        out_specs=VM,
        compiler_params=pltpu.CompilerParams(vmem_limit_bytes=VMEM_LIMIT),
        name="combine",
    )(target, route_weight.T, returned.reshape(N_EP * CAP, COLS))

    return (mixer_out, moe_out)


def solution(mesh):
    in_specs = (
        P("ep", None),
        P("ep", None),
        P("ep", None),
        P(),
        P(),
        P(None, "tp"),
        P(None, "tp"),
        P(None, "tp"),
        P(None, "tp"),
        P("tp", None),
        P("ep", None),
        P(),
        P("ep", None),
        P("ep", None),
        P("ep", None, "tp"),
        P("ep", None, "tp"),
        P("ep", "tp", None),
    )
    out_specs = (P(("ep", "tp"), None), P("ep", "tp"))
    return jax.shard_map(body, mesh=mesh, in_specs=in_specs, out_specs=out_specs, check_vma=False)
```

```python
import math

import jax
import jax.numpy as jnp
import numpy as np
from jax import lax
from jax.experimental import pallas as pl
from jax.experimental.pallas import tpu as pltpu
from jax.sharding import PartitionSpec as P

NOPE = 128
ROPE = 64
GRID_W = 64
epsilon = 1e-06
rotary_base = 10000.0
LOG2E = 1.4426950408889634
SCORE_SCALE = (NOPE + ROPE) ** (-0.5)

F32 = jnp.float32
BF16 = jnp.bfloat16
MESH = pl.DeviceIdType.MESH

N_EP = 64
N_TP = 4
PER_Z = 8
N_Z = 8
CAP = 16
COLS = 512
CHUNK = PER_Z * CAP
HALF = CHUNK // 2
VMEM_LIMIT = 62 * 1024 * 1024


def rotary_consts():
    inverse = np.float32(rotary_base) ** (-np.arange(0, 32, 2, dtype=np.float32) / np.float32(32))
    inverse = inverse.astype(np.float32)
    entry = np.arange(128) % ROPE
    pair = entry // 2
    row_lane = pair < 16
    freq = inverse[pair % 16]
    row_angle = (np.arange(128, dtype=np.float32)[:, None] * freq[None, :]).astype(np.float32)
    col_angle = (np.arange(64, dtype=np.float32)[:, None] * freq[None, :]).astype(np.float32)

    def both(angle, keep):
        wide = angle.astype(np.float64)
        return [np.where(keep, fn(wide), 0.0).astype(np.float32) for fn in (np.cos, np.sin)]

    row_cos, row_sin = both(row_angle, row_lane[None, :])
    col_cos, col_sin = both(col_angle, ~row_lane[None, :])
    rows = np.stack([row_cos.reshape(64, 2, 128), row_sin.reshape(64, 2, 128)], axis=1)
    rows = rows.reshape(64, 4, 128)
    cols = np.stack([col_cos, col_sin], axis=0)
    return rows, cols


def cos_sin(rows_ref, cols_ref, ep):
    rows = rows_ref[ep]
    cos = jnp.concatenate([rows[0:1] + cols_ref[0], rows[1:2] + cols_ref[0]], axis=0)
    sin = jnp.concatenate([rows[2:3] + cols_ref[1], rows[3:4] + cols_ref[1]], axis=0)
    return cos, sin


def turn(x, cos, sin):
    lane = lax.broadcasted_iota(jnp.int32, x.shape, 1)
    swapped = jnp.where(lane % 2 == 0, -pltpu.roll(x, 127, 1), pltpu.roll(x, 1, 1))
    return x * cos + swapped * sin


def rms(x, gain):
    wide = x.astype(F32)
    normed = wide * lax.rsqrt(jnp.mean(wide * wide, axis=-1, keepdims=True) + epsilon)
    return (normed * gain).astype(BF16)


NT = (((1,), (1,)), ((), ()))


ORDER_BENDS = ((2, 6), (-2, 5), (1, 4), (-4, 3), (3, 2))


def chunk_offset(c):
    bend = sum(k * ((c + start) // 8) for k, start in ORDER_BENDS)
    return c + bend


def all_columns(c):
    return c == 0


def latent_offset(a):
    return (a % 2) * ((a + 1) // 2) + (1 - a % 2) * ((8 - a // 2) % 8)


def remote(src, dst, send, recv, where):
    return pltpu.make_async_remote_copy(
        src_ref=src, dst_ref=dst, send_sem=send, recv_sem=recv, device_id=where, device_id_type=MESH
    )


def main_kernel(
    gain_ref, route_ref, weight_ref, klat_ref, rope_ref, kgain_ref, qlat_ref, qgain_ref, rows_ref, cols_ref,
    tok_hbm, wg_hbm, wu_hbm, wd_hbm, wq_hbm, wqr_hbm, wk_hbm, wv_hbm, wo_hbm,
    moe_ref, mixed_ref,
    tok, wg, wu, wq, wqr, wk, wv, wo, wdq, relay_p, relay_m,
    normed, outg, arr, hid, res, ret, columned, lat, query, qrot, top, total, acc, mix, got,
    wsem, send, rwd, rmix, ra2a, ry0p, ry0m, rfwp, rfwm, rh0p, rh0m, rhfp, rhfm, rret, rlz, rlxp, rlxm, rlfp, rlfm, rld,
):
    ep = lax.axis_index("ep")
    tp = lax.axis_index("tp")
    z = ep // PER_Z
    xc = ep % PER_Z
    x = xc // 2
    core = xc % 2
    up = (tp + 1) % N_TP
    down = (tp + N_TP - 1) % N_TP
    across = (tp + 2) % N_TP

    barrier = pltpu.get_barrier_semaphore()

    @pl.loop(1, N_EP)
    def _(i):
        pl.semaphore_signal(
            barrier, inc=1, device_id={"ep": (ep + i) % N_EP}, device_id_type=MESH
        )

    for other in (up, down, across):
        pl.semaphore_signal(barrier, inc=1, device_id={"tp": other}, device_id_type=MESH)

    def columns(which):
        return pl.ds(pl.multiple_of(which * COLS, COLS), COLS)

    pairs = (
        (tok_hbm, tok), (wd_hbm.at[:, columns(tp)], wdq.at[tp]), (wg_hbm, wg), (wu_hbm, wu),
        (wq_hbm, wq), (wqr_hbm, wqr), (wk_hbm, wk), (wv_hbm, wv), (wo_hbm, wo),
    )
    loads = [pltpu.make_async_copy(src, dst, wsem.at[i]) for i, (src, dst) in enumerate(pairs)]
    for load in loads:
        load.start()

    cos, sin = cos_sin(rows_ref, cols_ref, ep)
    lat[core, z, x, 0:128, :] = rms(klat_ref[...], kgain_ref[...])
    rope = rope_ref[...].astype(F32)
    rope = jnp.concatenate([rope, rope], axis=0).T
    turned = turn(rope, cos, sin)
    low = lax.broadcasted_iota(jnp.int32, (32, 128), 1) < ROPE
    left = jnp.where(low, turned[0:32], turned[32:64])
    right = jnp.where(low, turned[64:96], turned[96:128])
    lat[core, z, x, 128:160, :] = jnp.concatenate([left, right], axis=1).astype(BF16)

    route = route_ref[...]
    first = route[0:1, :]
    second = route[1:2, :]
    ids = lax.broadcasted_iota(jnp.int32, (N_EP, 512), 0)
    hit0 = (ids == first).astype(F32)
    hit1 = (ids == second).astype(F32)
    before = lax.broadcasted_iota(jnp.int32, (512, 512), 0) < lax.broadcasted_iota(
        jnp.int32, (512, 512), 1
    )
    earlier = jnp.dot((hit0 + hit1).astype(BF16), before.astype(BF16), preferred_element_type=F32)
    slot0 = jnp.sum(hit0 * earlier, axis=0, keepdims=True).astype(jnp.int32)
    slot1 = jnp.sum(hit1 * earlier, axis=0, keepdims=True).astype(jnp.int32)
    target0 = first * CAP + slot0
    target1 = second * CAP + slot1

    loads[0].wait()

    @pl.loop(0, 8)
    def _(i):
        sel = pl.ds(pl.multiple_of(i * 64, 64), 64)
        wide = tok[sel, :].astype(F32)
        scale = lax.rsqrt(jnp.mean(wide * wide, axis=-1, keepdims=True) + epsilon)
        normed[sel, :] = (wide * scale * gain_ref[...]).astype(BF16)

    pl.semaphore_wait(barrier, N_EP - 1 + 3)

    def y_copy(src, dst, send_at, recv, where):
        return remote(src, dst, send.at[send_at], recv, {"tp": where})

    y_copy(wd_hbm.at[:, columns(up)], wdq.at[tp], 0, rwd.at[0], up).start()
    y_copy(wd_hbm.at[:, columns(down)], wdq.at[tp], 1, rwd.at[1], down).start()
    y_copy(wd_hbm.at[pl.ds(0, 128), columns(across)], relay_p, 2, rwd.at[2], up).start()
    y_copy(wd_hbm.at[pl.ds(128, 128), columns(across)], relay_m, 3, rwd.at[3], down).start()

    def latent_plane(a):
        return (z + N_Z - latent_offset(a)) % N_Z

    def ep_at(z_at, x_at):
        return ((z_at + N_Z) % N_Z) * PER_Z + ((x_at + 4) % 4) * 2 + core

    def latents_x(a):
        block = lat.at[core, latent_plane(a), x]

        def along_z(step, which):
            remote(block, block, send.at[7], rlz.at[which], {"ep": ep_at(z + step, x)}).start()

        @pl.when(a != 0)
        def _():
            remote(block, block, send.at[7], rlz.at[a], {"tp": up}).wait_recv()

        @pl.when(a == 0)
        def _():
            along_z(1, 1)
            along_z(-1, 2)

        @pl.when((a % 2 == 1) & (a < 7))
        def _():
            along_z(1, a + 2)

        @pl.when((a % 2 == 0) & (a > 0) & (a < 6))
        def _():
            along_z(-1, a + 2)

        remote(block, block, send.at[17], rlxp.at[a], {"ep": ep_at(z, x + 1)}).start()
        remote(block, block, send.at[17], rlxm.at[a], {"ep": ep_at(z, x - 1)}).start()

    def latents_on(a):
        at = latent_plane(a)
        below = lat.at[core, at, (x + 3) % 4]
        remote(below, below, send.at[17], rlxp.at[a], {"tp": up}).wait_recv()
        half = lat.at[core, at, (x + 3) % 4, pl.ds(0, 80)]
        remote(half, half, send.at[22], rlfp.at[a], {"ep": ep_at(z, x + 1)}).start()
        above = lat.at[core, at, (x + 1) % 4]
        remote(above, above, send.at[17], rlxm.at[a], {"tp": up}).wait_recv()
        half = lat.at[core, at, (x + 1) % 4, pl.ds(80, 80)]
        remote(half, half, send.at[22], rlfm.at[a], {"ep": ep_at(z, x - 1)}).start()

    def latents_core(a):
        at = latent_plane(a)
        half = lat.at[core, at, (x + 2) % 4, pl.ds(0, 80)]
        remote(half, half, send.at[22], rlfp.at[a], {"tp": up}).wait_recv()
        half = lat.at[core, at, (x + 2) % 4, pl.ds(80, 80)]
        remote(half, half, send.at[22], rlfm.at[a], {"tp": up}).wait_recv()
        four = lat.at[core, at]
        remote(four, four, send.at[18], rld.at[a], {"ep": z * PER_Z + x * 2 + (1 - core)}).start()

    latents_x(0)

    def rows_out(c):
        zd = (z + chunk_offset(c)) % N_Z
        far = zd * PER_Z
        ids = lax.broadcasted_iota(jnp.int32, (CHUNK, 512), 0) + zd * CHUNK
        pick = ((ids == target0) | (ids == target1)).astype(BF16)

        def take(q):
            rows = jnp.dot(pick, normed[:, columns(q)], preferred_element_type=F32).astype(BF16)
            outg[q, pl.ds(far, PER_Z)] = rows.reshape(PER_Z, CAP, COLS)

        @pl.when(all_columns(c))
        def _():
            for q in range(N_TP):
                take(q)

            def put(other):
                remote(
                    outg.at[:, other], arr.at[:, ep], send.at[23], ra2a.at[c], {"ep": other}
                ).start()

            @pl.loop(1, PER_Z)
            def _(j):
                put(far + (xc + j) % PER_Z)

        @pl.when(jnp.logical_not(all_columns(c)))
        def _():
            take(tp)

            @pl.loop(0, PER_Z)
            def _(j):
                other = far + (xc + j) % PER_Z
                remote(
                    outg.at[tp, other], arr.at[tp, ep], send.at[6], ra2a.at[c], {"ep": other}
                ).start()

    @pl.loop(0, N_Z)
    def _(i):
        rows_out(i + (7 - i) // 7 - (8 - i) // 7 + (8 - i) // 8)

    arr[:, pl.ds(ep, 1)] = outg[:, pl.ds(ep, 1)]

    for load in loads[1:]:
        load.wait()

    qn = rms(qlat_ref[...], qgain_ref[...])
    nope = jnp.dot(qn, wq[...], preferred_element_type=F32).astype(BF16)
    for h in range(2):
        sel = slice(h * 128, (h + 1) * 128)
        query[sel, :] = lax.dot_general(
            nope[:, sel], wk[:, sel], NT, preferred_element_type=F32
        ).astype(BF16)
    rot = turn(jnp.dot(qn, wqr[...], preferred_element_type=F32), cos, sin)
    low = lax.broadcasted_iota(jnp.int32, (128, 128), 1) < ROPE
    rolled = pltpu.roll(rot, ROPE, 1)
    near = jnp.concatenate([jnp.where(low, rot, 0.0), jnp.where(low, rolled, 0.0)], axis=0)
    far = jnp.concatenate([jnp.where(low, 0.0, rolled), jnp.where(low, 0.0, rot)], axis=0)
    near = near.astype(BF16)
    far = far.astype(BF16)
    none = jnp.zeros((256, 128), BF16)
    for g, pair in enumerate(((near, none), (far, none), (none, near), (none, far))):
        qrot[g] = jnp.concatenate(pair, axis=1)
    columned[...] = jnp.concatenate(
        [target0.astype(F32), target1.astype(F32), weight_ref[...], jnp.zeros((124, 512), F32)], axis=0
    ).T
    moe_ref[...] = jnp.zeros((512, COLS), F32)
    top[...] = jnp.full((256, 1), -1e30, F32)
    total[...] = jnp.zeros((256, 1), F32)
    acc[...] = jnp.zeros((256, 256), F32)

    def plane(c):
        return (z + N_Z - chunk_offset(c)) % N_Z

    def tokens_in(c):
        at = plane(c) * PER_Z
        whole = arr.at[tp, pl.ds(at, PER_Z)]
        remote(whole, whole, send.at[6], ra2a.at[c], {"tp": up}).wait_recv()
        y_copy(whole, whole, 8, ry0p.at[c], up).start()
        y_copy(whole, whole, 9, ry0m.at[c], down).start()

    def tokens_on(c):
        at = plane(c) * PER_Z
        below = arr.at[down, pl.ds(at, PER_Z)]
        above = arr.at[up, pl.ds(at, PER_Z)]
        y_copy(below, below, 8, ry0p.at[c], up).wait_recv()
        half = arr.at[down, pl.ds(at, PER_Z // 2)]
        y_copy(half, half, 10, rfwp.at[c], up).start()
        y_copy(above, above, 9, ry0m.at[c], down).wait_recv()
        half = arr.at[up, pl.ds(at + PER_Z // 2, PER_Z // 2)]
        y_copy(half, half, 11, rfwm.at[c], down).start()

    def hidden_units(c):
        at = plane(c) * PER_Z

        @pl.when(c == 0)
        def _():
            less = arr.at[:, pl.ds(0, PER_Z - 1)]
            remote(less, less, send.at[23], ra2a.at[c], {"tp": up}).wait_recv()

        @pl.when(jnp.logical_not(all_columns(c)))
        def _():
            half = arr.at[across, pl.ds(at, PER_Z // 2)]
            y_copy(half, half, 10, rfwp.at[c], up).wait_recv()
            half = arr.at[across, pl.ds(at + PER_Z // 2, PER_Z // 2)]
            y_copy(half, half, 11, rfwm.at[c], down).wait_recv()

        gate = jnp.zeros((CHUNK, 256), F32)
        upper = jnp.zeros((CHUNK, 256), F32)
        for q in range(N_TP):
            rows = arr[q, pl.ds(at, PER_Z)].reshape(CHUNK, COLS)
            gate += jnp.dot(rows, wg[q * COLS : (q + 1) * COLS, :], preferred_element_type=F32)
            upper += jnp.dot(rows, wu[q * COLS : (q + 1) * COLS, :], preferred_element_type=F32)
        hid[c, tp] = (gate / (1.0 + jnp.exp(-gate)) * upper).astype(BF16)
        mine = hid.at[c, tp]
        y_copy(mine, mine, 12, rh0p.at[c], up).start()
        y_copy(mine, mine, 13, rh0m.at[c], down).start()

    def hidden_on(c):
        y_copy(hid.at[c, down], hid.at[c, down], 12, rh0p.at[c], up).wait_recv()
        half = hid.at[c, down, pl.ds(0, HALF)]
        y_copy(half, half, 14, rhfp.at[c], up).start()
        y_copy(hid.at[c, up], hid.at[c, up], 13, rh0m.at[c], down).wait_recv()
        half = hid.at[c, up, pl.ds(HALF, HALF)]
        y_copy(half, half, 15, rhfm.at[c], down).start()

    def results_out(c):
        at = plane(c) * PER_Z

        @pl.when(c == 0)
        def _():
            whole = wdq.at[0]
            half = wdq.at[0, pl.ds(0, 128)]
            y_copy(whole, whole, 0, rwd.at[0], up).wait_recv()
            y_copy(whole, whole, 1, rwd.at[1], down).wait_recv()
            y_copy(half, half, 4, rwd.at[4], up).wait_recv()
            y_copy(half, half, 5, rwd.at[5], down).wait_recv()

        half = hid.at[c, across, pl.ds(0, HALF)]
        y_copy(half, half, 14, rhfp.at[c], up).wait_recv()
        half = hid.at[c, across, pl.ds(HALF, HALF)]
        y_copy(half, half, 15, rhfm.at[c], down).wait_recv()
        sums = jnp.zeros((CHUNK, COLS), F32)
        for q in range(N_TP):
            term = jnp.dot(hid[c, q], wdq[q], preferred_element_type=F32)
            sums += term.astype(BF16).astype(F32)
        res[c] = sums.astype(BF16).reshape(PER_Z, CAP, COLS)

        def put(j):
            remote(
                res.at[c, j], ret.at[ep], send.at[16], rret.at[c], {"ep": at + j}
            ).start()

        @pl.when(c != 0)
        def _():
            put(xc)

        @pl.when(c == 0)
        def _():
            ret[pl.ds(ep, 1)] = res[c, pl.ds(xc, 1)]

        @pl.loop(1, PER_Z)
        def _(j):
            put((xc + j) % PER_Z)

    def combine(c):
        far = ((z + chunk_offset(c)) % N_Z) * PER_Z
        whole = ret.at[pl.ds(far, PER_Z)]
        less = ret.at[pl.ds(0, PER_Z - 1)]

        @pl.when(c == 0)
        def _():
            remote(less, less, send.at[16], rret.at[c], {"tp": up}).wait_recv()

        @pl.when(c != 0)
        def _():
            remote(whole, whole, send.at[16], rret.at[c], {"tp": up}).wait_recv()

        ids = (lax.broadcasted_iota(jnp.int32, (128, CHUNK), 1) + far * CAP).astype(F32)
        back = ret[pl.ds(far, PER_Z)].reshape(CHUNK, COLS)

        for i in range(4):
            sel = slice(i * 128, (i + 1) * 128)
            sums = moe_ref[sel, :]
            for k in range(2):
                pick = (ids == columned[sel, k : k + 1]).astype(BF16)
                got_rows = jnp.dot(pick, back, preferred_element_type=F32)
                sums += got_rows * columned[sel, 2 + k : 3 + k]
            moe_ref[sel, :] = sums

    def relay(c):
        y_copy(relay_p, relay_p, 2, rwd.at[2], up).wait_recv()
        y_copy(relay_p, wdq.at[down, pl.ds(0, 128)], 4, rwd.at[4], up).start()
        y_copy(relay_m, relay_m, 3, rwd.at[3], down).wait_recv()
        y_copy(relay_m, wdq.at[up, pl.ds(128, 128)], 5, rwd.at[5], down).start()

    def attend(c):
        at = latent_plane(c)
        four = lat.at[1 - core, at]
        remote(four, four, send.at[18], rld.at[c], {"tp": up}).wait_recv()
        turned = lat[:, at, :, 128:160, :].reshape(256, 256)
        keys = []
        scores = []
        for g in range(4):
            keys.append(lat[:, at, :, g * 32 : (g + 1) * 32, :].reshape(256, 256))
            s = lax.dot_general(query[...], keys[g], NT, preferred_element_type=F32)
            s += lax.dot_general(qrot[g], turned, NT, preferred_element_type=F32)
            scores.append(s * (SCORE_SCALE * LOG2E))
        peak = jnp.maximum(
            jnp.maximum(scores[0], scores[1]), jnp.maximum(scores[2], scores[3])
        )
        new_top = jnp.maximum(top[...], jnp.max(peak, axis=1, keepdims=True))
        fade = jnp.exp2(top[...] - new_top)
        weighed = acc[...] * fade
        sums = jnp.zeros((256, 256), F32)
        for g in range(4):
            weights = jnp.exp2(scores[g] - new_top)
            sums += weights
            weighed += jnp.dot(weights.astype(BF16), keys[g], preferred_element_type=F32)
        total[...] = total[...] * fade + jnp.sum(sums, axis=1, keepdims=True)
        acc[...] = weighed
        top[...] = new_top

    def mix_copy(i):
        other = (tp + i) % N_TP
        return remote(mix.at[other], got.at[i], send.at[18 + i], rmix.at[i], {"tp": other})

    def project(c):
        mean = (acc[...] / total[...]).astype(BF16)
        heads = []
        for h in range(2):
            sel = slice(h * 128, (h + 1) * 128)
            heads.append(
                jnp.dot(mean[sel], wv[:, sel], preferred_element_type=F32).astype(BF16)
            )
        heads = jnp.concatenate(heads, axis=1)
        for q in range(4):
            sel = slice(q * 512, (q + 1) * 512)
            term = jnp.dot(heads, wo[:, sel], preferred_element_type=F32)
            mix[:, :, sel] = term.astype(BF16).reshape(N_TP, 32, 512)
        for i in range(1, N_TP):
            mix_copy(i).start()

    def twice(stage, start):
        def both(c):
            stage(start + 2 * c)
            stage(start + 1 + 2 * c)

        both.__name__ = stage.__name__
        return both

    def after(stage, start):
        def later(c):
            stage(start + c)

        later.__name__ = stage.__name__
        return later

    plan = (
        (0, 7, after(tokens_in, 1)),
        (0, 1, relay),
        (1, 7, after(tokens_on, 1)),
        (1, 8, hidden_units),
        (2, 8, hidden_on),
        (3, 8, results_out),
        (0, 3, after(latents_x, 1)),
        (3, 2, twice(latents_x, 4)),
        (0, 4, latents_on),
        (4, 2, twice(latents_on, 4)),
        (1, 4, latents_core),
        (5, 2, twice(latents_core, 4)),
        (2, 4, attend),
        (6, 2, twice(attend, 4)),
        (9, 1, project),
        (6, N_Z, combine),
    )

    @pl.loop(0, 14)
    def _(i):
        for lag, count, stage in plan:

            @pl.when((i >= lag) & (i < lag + count))
            def _(stage=stage, lag=lag):
                stage(i - lag)

    sums = mix[tp].astype(F32)
    for i in range(1, N_TP):
        mix_copy(i).wait()
        sums = sums + got[i].astype(F32)
    mixed_ref[...] = sums

    def sent(ref, which):
        remote(ref, ref, send.at[which], ra2a.at[0], {"tp": up}).wait_send()

    for which in (0, 1):
        sent(wdq.at[0], which)
    for which in (2, 3, 4, 5):
        sent(relay_p, which)
    sent(outg.at[0, pl.ds(0, 56)], 6)
    sent(outg.at[:, pl.ds(0, 7)], 23)
    sent(lat.at[0, pl.ds(0, 7), 0], 7)
    for which in (8, 9):
        sent(arr.at[0, pl.ds(0, 56)], which)
    for which in (10, 11):
        sent(arr.at[0, pl.ds(0, 28)], which)
    for which in (12, 13):
        sent(hid.at[:, 0], which)
    for which in (14, 15):
        sent(hid.at[:, 0, pl.ds(0, HALF)], which)
    sent(ret.at[pl.ds(0, N_EP - 1)], 16)
    sent(lat.at[0, :, pl.ds(0, 2)], 17)
    sent(lat.at[0, :, 0], 22)
    sent(lat.at[0], 18)


def finish_kernel(moe_ref, mixed_ref, moe_out, mixed_out):
    moe_out[...] = moe_ref[...].astype(BF16)
    mixed_out[...] = mixed_ref[...].astype(BF16)


VM = pl.BlockSpec(memory_space=pltpu.VMEM)
ANY = pl.BlockSpec(memory_space=pl.ANY)


def struct(shape, dtype=BF16):
    return jax.ShapeDtypeStruct(shape, dtype)


def body(
    query_latent, key_latent, rope_key, query_gain, key_gain, w_query, w_query_rope, w_key,
    w_value, w_out, tokens_b, ffn_gain, route_expert, route_weight, w_gate, w_up, w_down,
):
    rows_np, cols_np = rotary_consts()
    rows = jnp.asarray(rows_np)
    cols = jnp.asarray(cols_np)
    dma = pltpu.SemaphoreType.DMA

    moe, mixed = pl.pallas_call(
        main_kernel,
        out_shape=(
            struct((512, COLS), F32),
            struct((32, 2048), F32),
        ),
        in_specs=[VM] * 10 + [ANY] * 9,
        out_specs=(VM, VM),
        scratch_shapes=[
            pltpu.VMEM(shape, dtype)
            for shape, dtype in (
                ((512, 2048), BF16),
                ((2048, 256), BF16),
                ((2048, 256), BF16),
                ((512, 256), BF16),
                ((512, 128), BF16),
                ((256, 256), BF16),
                ((256, 256), BF16),
                ((256, 2048), BF16),
                ((N_TP, 256, COLS), BF16),
                ((128, COLS), BF16),
                ((128, COLS), BF16),
                ((512, 2048), BF16),
                ((N_TP, N_EP, CAP, COLS), BF16),
                ((N_TP, N_EP, CAP, COLS), BF16),
                ((N_Z, N_TP, CHUNK, 256), BF16),
                ((N_Z, PER_Z, CAP, COLS), BF16),
                ((N_EP, CAP, COLS), BF16),
                ((512, 128), F32),
                ((2, N_Z, 4, 160, 256), BF16),
                ((256, 256), BF16),
                ((4, 256, 256), BF16),
                ((256, 1), F32),
                ((256, 1), F32),
                ((256, 256), F32),
                ((N_TP, 32, 2048), BF16),
                ((N_TP, 32, 2048), BF16),
            )
        ]
        + [dma((9,)), dma((24,)), dma((6,)), dma((N_TP,))]
        + [dma((N_Z,))] * 16,
        compiler_params=pltpu.CompilerParams(
            collective_id=0, has_side_effects=True, vmem_limit_bytes=VMEM_LIMIT
        ),
        name="exchange",
    )(
        ffn_gain.reshape(1, -1), route_expert.T, route_weight.T, key_latent, rope_key.T, key_gain.reshape(1, -1),
        query_latent, query_gain.reshape(1, -1), rows, cols,
        tokens_b, w_gate[0], w_up[0], w_down[0], w_query, w_query_rope, w_key, w_value, w_out,
    )

    moe_out, mixer_out = pl.pallas_call(
        finish_kernel,
        out_shape=(struct((512, COLS)), struct((32, 2048))),
        in_specs=[VM] * 2,
        out_specs=(VM, VM),
        compiler_params=pltpu.CompilerParams(vmem_limit_bytes=VMEM_LIMIT),
        name="finish",
    )(moe, mixed)

    return (mixer_out, moe_out)


def solution(mesh):
    in_specs = (
        P("ep", None),
        P("ep", None),
        P("ep", None),
        P(),
        P(),
        P(None, "tp"),
        P(None, "tp"),
        P(None, "tp"),
        P(None, "tp"),
        P("tp", None),
        P("ep", None),
        P(),
        P("ep", None),
        P("ep", None),
        P("ep", None, "tp"),
        P("ep", None, "tp"),
        P("ep", "tp", None),
    )
    out_specs = (P(("ep", "tp"), None), P("ep", "tp"))
    return jax.shard_map(body, mesh=mesh, in_specs=in_specs, out_specs=out_specs, check_vma=False)
```

```python
import math

import jax
import jax.numpy as jnp
import numpy as np
from jax import lax
from jax.experimental import pallas as pl
from jax.experimental.pallas import tpu as pltpu
from jax.sharding import PartitionSpec as P

NOPE = 128
ROPE = 64
GRID_W = 64
epsilon = 1e-06
rotary_base = 10000.0
LOG2E = 1.4426950408889634
SCORE_SCALE = (NOPE + ROPE) ** (-0.5)

F32 = jnp.float32
BF16 = jnp.bfloat16
MESH = pl.DeviceIdType.MESH

N_EP = 64
N_TP = 4
PER_Z = 8
N_Z = 8
CAP = 16
COLS = 512
CHUNK = PER_Z * CAP
HALF = CHUNK // 2
VMEM_LIMIT = 62 * 1024 * 1024


def rotary_consts():
    inverse = np.float32(rotary_base) ** (-np.arange(0, 32, 2, dtype=np.float32) / np.float32(32))
    inverse = inverse.astype(np.float32)
    entry = np.arange(128) % ROPE
    pair = entry // 2
    row_lane = pair < 16
    freq = inverse[pair % 16]
    row_angle = (np.arange(128, dtype=np.float32)[:, None] * freq[None, :]).astype(np.float32)
    col_angle = (np.arange(64, dtype=np.float32)[:, None] * freq[None, :]).astype(np.float32)

    def both(angle, keep):
        wide = angle.astype(np.float64)
        return [np.where(keep, fn(wide), 0.0).astype(np.float32) for fn in (np.cos, np.sin)]

    row_cos, row_sin = both(row_angle, row_lane[None, :])
    col_cos, col_sin = both(col_angle, ~row_lane[None, :])
    rows = np.stack([row_cos.reshape(64, 2, 128), row_sin.reshape(64, 2, 128)], axis=1)
    rows = rows.reshape(64, 4, 128)
    cols = np.stack([col_cos, col_sin], axis=0)
    return rows, cols


def cos_sin(rows_ref, cols_ref):
    rows = rows_ref[...]
    cos = jnp.concatenate([rows[0:1] + cols_ref[0], rows[1:2] + cols_ref[0]], axis=0)
    sin = jnp.concatenate([rows[2:3] + cols_ref[1], rows[3:4] + cols_ref[1]], axis=0)
    return cos, sin


def turn(x, cos, sin):
    lane = lax.broadcasted_iota(jnp.int32, x.shape, 1)
    swapped = jnp.where(lane % 2 == 0, -pltpu.roll(x, 127, 1), pltpu.roll(x, 1, 1))
    return x * cos + swapped * sin


def rms(x, gain):
    wide = x.astype(F32)
    normed = wide * lax.rsqrt(jnp.mean(wide * wide, axis=-1, keepdims=True) + epsilon)
    return (normed * gain).astype(BF16)


NT = (((1,), (1,)), ((), ()))


ORDER_BENDS = ((1, 7), (2, 6), (-3, 5), (1, 3), (-6, 2), (5, 1))


def chunk_offset(c):
    bend = sum(k * ((c + start) // 8) for k, start in ORDER_BENDS)
    return c + bend


def all_columns(c):
    return c == 0


def latent_offset(a):
    return (a % 2) * ((a + 1) // 2) + (1 - a % 2) * ((8 - a // 2) % 8)


def remote(src, dst, send, recv, where):
    return pltpu.make_async_remote_copy(
        src_ref=src, dst_ref=dst, send_sem=send, recv_sem=recv, device_id=where, device_id_type=MESH
    )


def main_kernel(
    gain_hbm, route_hbm, weight_hbm, klat_hbm, rope_hbm, kgain_hbm, qlat_hbm, qgain_hbm, rows_hbm, cols_hbm,
    tok_hbm, wg_hbm, wu_hbm, wd_hbm, wq_hbm, wqr_hbm, wk_hbm, wv_hbm, wo_hbm,
    moe_ref, mixed_ref,
    gain_ref, route_ref, weight_ref, klat_ref, rope_ref, kgain_ref, qlat_ref, qgain_ref, rows_ref, cols_ref,
    tok, wg, wu, wq, wqr, wk, wv, wo, wdq, relay_p, relay_m,
    normed, outg, arr, hid, res, ret, columned, lat, query, qrot, top, total, acc, mix, got,
    wsem, send, rwd, rmix, ra2a, ry0p, ry0m, rfwp, rfwm, rh0p, rh0m, rhfp, rhfm, rret, rlz, rlxp, rlxm, rlfp, rlfm, rld,
):
    ep = lax.axis_index("ep")
    tp = lax.axis_index("tp")
    z = ep // PER_Z
    xc = ep % PER_Z
    x = xc // 2
    core = xc % 2
    up = (tp + 1) % N_TP
    down = (tp + N_TP - 1) % N_TP
    across = (tp + 2) % N_TP

    barrier = pltpu.get_barrier_semaphore()

    @pl.loop(1, N_EP)
    def _(i):
        pl.semaphore_signal(
            barrier, inc=1, device_id={"ep": (ep + i) % N_EP}, device_id_type=MESH
        )

    for other in (up, down, across):
        pl.semaphore_signal(barrier, inc=1, device_id={"tp": other}, device_id_type=MESH)

    def columns(which):
        return pl.ds(pl.multiple_of(which * COLS, COLS), COLS)

    pairs = (
        (klat_hbm, klat_ref), (kgain_hbm, kgain_ref), (rope_hbm, rope_ref),
        (rows_hbm.at[ep], rows_ref), (cols_hbm, cols_ref), (route_hbm, route_ref),
        (gain_hbm, gain_ref), (tok_hbm, tok), (weight_hbm, weight_ref), (qlat_hbm, qlat_ref),
        (qgain_hbm, qgain_ref), (wd_hbm.at[:, columns(tp)], wdq.at[tp]), (wg_hbm, wg), (wu_hbm, wu),
        (wq_hbm, wq), (wqr_hbm, wqr), (wk_hbm, wk), (wv_hbm, wv), (wo_hbm, wo),
    )
    loads = [pltpu.make_async_copy(src, dst, wsem.at[i]) for i, (src, dst) in enumerate(pairs)]
    for load in loads:
        load.start()

    for load in loads[0:6]:
        load.wait()

    cos, sin = cos_sin(rows_ref, cols_ref)
    lat[core, z, x, 0:128, :] = rms(klat_ref[...], kgain_ref[...])
    rope = rope_ref[...].astype(F32)
    rope = jnp.concatenate([rope, rope], axis=0).T
    turned = turn(rope, cos, sin)
    low = lax.broadcasted_iota(jnp.int32, (32, 128), 1) < ROPE
    left = jnp.where(low, turned[0:32], turned[32:64])
    right = jnp.where(low, turned[64:96], turned[96:128])
    lat[core, z, x, 128:160, :] = jnp.concatenate([left, right], axis=1).astype(BF16)

    route = route_ref[...]
    first = route[0:1, :]
    second = route[1:2, :]
    ids = lax.broadcasted_iota(jnp.int32, (N_EP, 512), 0)
    hit0 = (ids == first).astype(F32)
    hit1 = (ids == second).astype(F32)
    before = lax.broadcasted_iota(jnp.int32, (512, 512), 0) < lax.broadcasted_iota(
        jnp.int32, (512, 512), 1
    )
    earlier = jnp.dot((hit0 + hit1).astype(BF16), before.astype(BF16), preferred_element_type=F32)
    slot0 = jnp.sum(hit0 * earlier, axis=0, keepdims=True).astype(jnp.int32)
    slot1 = jnp.sum(hit1 * earlier, axis=0, keepdims=True).astype(jnp.int32)
    target0 = first * CAP + slot0
    target1 = second * CAP + slot1

    pl.semaphore_wait(barrier, N_EP - 1 + 3)

    def y_copy(src, dst, send_at, recv, where):
        return remote(src, dst, send.at[send_at], recv, {"tp": where})

    y_copy(wd_hbm.at[:, columns(up)], wdq.at[tp], 0, rwd.at[0], up).start()
    y_copy(wd_hbm.at[:, columns(down)], wdq.at[tp], 1, rwd.at[1], down).start()
    y_copy(wd_hbm.at[pl.ds(0, 128), columns(across)], relay_p, 2, rwd.at[2], up).start()
    y_copy(wd_hbm.at[pl.ds(128, 128), columns(across)], relay_m, 3, rwd.at[3], down).start()

    def latent_plane(a):
        return (z + N_Z - latent_offset(a)) % N_Z

    def ep_at(z_at, x_at):
        return ((z_at + N_Z) % N_Z) * PER_Z + ((x_at + 4) % 4) * 2 + core

    def latents_x(a):
        block = lat.at[core, latent_plane(a), x]

        def along_z(step, which):
            remote(block, block, send.at[7], rlz.at[which], {"ep": ep_at(z + step, x)}).start()

        @pl.when(a != 0)
        def _():
            remote(block, block, send.at[7], rlz.at[a], {"tp": up}).wait_recv()

        @pl.when(a == 0)
        def _():
            along_z(1, 1)
            along_z(-1, 2)

        @pl.when((a % 2 == 1) & (a < 7))
        def _():
            along_z(1, a + 2)

        @pl.when((a % 2 == 0) & (a > 0) & (a < 6))
        def _():
            along_z(-1, a + 2)

        remote(block, block, send.at[17], rlxp.at[a], {"ep": ep_at(z, x + 1)}).start()
        remote(block, block, send.at[17], rlxm.at[a], {"ep": ep_at(z, x - 1)}).start()

    def latents_on(a):
        at = latent_plane(a)
        below = lat.at[core, at, (x + 3) % 4]
        remote(below, below, send.at[17], rlxp.at[a], {"tp": up}).wait_recv()
        half = lat.at[core, at, (x + 3) % 4, pl.ds(0, 80)]
        remote(half, half, send.at[22], rlfp.at[a], {"ep": ep_at(z, x + 1)}).start()
        above = lat.at[core, at, (x + 1) % 4]
        remote(above, above, send.at[17], rlxm.at[a], {"tp": up}).wait_recv()
        half = lat.at[core, at, (x + 1) % 4, pl.ds(80, 80)]
        remote(half, half, send.at[22], rlfm.at[a], {"ep": ep_at(z, x - 1)}).start()

    def latents_core(a):
        at = latent_plane(a)
        half = lat.at[core, at, (x + 2) % 4, pl.ds(0, 80)]
        remote(half, half, send.at[22], rlfp.at[a], {"tp": up}).wait_recv()
        half = lat.at[core, at, (x + 2) % 4, pl.ds(80, 80)]
        remote(half, half, send.at[22], rlfm.at[a], {"tp": up}).wait_recv()
        four = lat.at[core, at]
        remote(four, four, send.at[18], rld.at[a], {"ep": z * PER_Z + x * 2 + (1 - core)}).start()

    latents_x(0)

    loads[6].wait()
    loads[7].wait()

    @pl.loop(0, 8)
    def _(i):
        sel = pl.ds(pl.multiple_of(i * 64, 64), 64)
        wide = tok[sel, :].astype(F32)
        scale = lax.rsqrt(jnp.mean(wide * wide, axis=-1, keepdims=True) + epsilon)
        normed[sel, :] = (wide * scale * gain_ref[...]).astype(BF16)

    def rows_out(c):
        zd = (z + chunk_offset(c)) % N_Z
        far = zd * PER_Z
        ids = lax.broadcasted_iota(jnp.int32, (CHUNK, 512), 0) + zd * CHUNK
        pick = ((ids == target0) | (ids == target1)).astype(BF16)

        def take(q):
            rows = jnp.dot(pick, normed[:, columns(q)], preferred_element_type=F32).astype(BF16)
            outg[q, pl.ds(far, PER_Z)] = rows.reshape(PER_Z, CAP, COLS)

        @pl.when(all_columns(c))
        def _():
            for q in range(N_TP):
                take(q)

            def put(other):
                remote(
                    outg.at[:, other], arr.at[:, ep], send.at[23], ra2a.at[c], {"ep": other}
                ).start()

            @pl.loop(1, PER_Z)
            def _(j):
                put(far + (xc + j) % PER_Z)

        @pl.when(jnp.logical_not(all_columns(c)))
        def _():
            take(tp)

            @pl.loop(0, PER_Z)
            def _(j):
                other = far + (xc + j) % PER_Z
                remote(
                    outg.at[tp, other], arr.at[tp, ep], send.at[6], ra2a.at[c], {"ep": other}
                ).start()

    @pl.loop(0, N_Z)
    def _(i):
        rows_out(i + (7 - i) // 7 - (8 - i) // 7 + (8 - i) // 8)

    arr[:, pl.ds(ep, 1)] = outg[:, pl.ds(ep, 1)]

    for load in loads[8:]:
        load.wait()

    qn = rms(qlat_ref[...], qgain_ref[...])
    nope = jnp.dot(qn, wq[...], preferred_element_type=F32).astype(BF16)
    for h in range(2):
        sel = slice(h * 128, (h + 1) * 128)
        query[sel, :] = lax.dot_general(
            nope[:, sel], wk[:, sel], NT, preferred_element_type=F32
        ).astype(BF16)
    rot = turn(jnp.dot(qn, wqr[...], preferred_element_type=F32), cos, sin)
    low = lax.broadcasted_iota(jnp.int32, (128, 128), 1) < ROPE
    rolled = pltpu.roll(rot, ROPE, 1)
    near = jnp.concatenate([jnp.where(low, rot, 0.0), jnp.where(low, rolled, 0.0)], axis=0)
    far = jnp.concatenate([jnp.where(low, 0.0, rolled), jnp.where(low, 0.0, rot)], axis=0)
    near = near.astype(BF16)
    far = far.astype(BF16)
    none = jnp.zeros((256, 128), BF16)
    for g, pair in enumerate(((near, none), (far, none), (none, near), (none, far))):
        qrot[g] = jnp.concatenate(pair, axis=1)
    columned[...] = jnp.concatenate(
        [target0.astype(F32), target1.astype(F32), weight_ref[...], jnp.zeros((124, 512), F32)], axis=0
    ).T
    moe_ref[...] = jnp.zeros((512, COLS), F32)
    top[...] = jnp.full((256, 1), -1e30, F32)
    total[...] = jnp.zeros((256, 1), F32)
    acc[...] = jnp.zeros((256, 256), F32)

    def plane(c):
        return (z + N_Z - chunk_offset(c)) % N_Z

    def tokens_in(c):
        at = plane(c) * PER_Z
        whole = arr.at[tp, pl.ds(at, PER_Z)]
        remote(whole, whole, send.at[6], ra2a.at[c], {"tp": up}).wait_recv()
        y_copy(whole, whole, 8, ry0p.at[c], up).start()
        y_copy(whole, whole, 9, ry0m.at[c], down).start()

    def tokens_on(c):
        at = plane(c) * PER_Z
        below = arr.at[down, pl.ds(at, PER_Z)]
        above = arr.at[up, pl.ds(at, PER_Z)]
        y_copy(below, below, 8, ry0p.at[c], up).wait_recv()
        half = arr.at[down, pl.ds(at, PER_Z // 2)]
        y_copy(half, half, 10, rfwp.at[c], up).start()
        y_copy(above, above, 9, ry0m.at[c], down).wait_recv()
        half = arr.at[up, pl.ds(at + PER_Z // 2, PER_Z // 2)]
        y_copy(half, half, 11, rfwm.at[c], down).start()

    def hidden_units(c):
        at = plane(c) * PER_Z

        @pl.when(c == 0)
        def _():
            less = arr.at[:, pl.ds(0, PER_Z - 1)]
            remote(less, less, send.at[23], ra2a.at[c], {"tp": up}).wait_recv()

        @pl.when(jnp.logical_not(all_columns(c)))
        def _():
            half = arr.at[across, pl.ds(at, PER_Z // 2)]
            y_copy(half, half, 10, rfwp.at[c], up).wait_recv()
            half = arr.at[across, pl.ds(at + PER_Z // 2, PER_Z // 2)]
            y_copy(half, half, 11, rfwm.at[c], down).wait_recv()

        gate = jnp.zeros((CHUNK, 256), F32)
        upper = jnp.zeros((CHUNK, 256), F32)
        for q in range(N_TP):
            rows = arr[q, pl.ds(at, PER_Z)].reshape(CHUNK, COLS)
            gate += jnp.dot(rows, wg[q * COLS : (q + 1) * COLS, :], preferred_element_type=F32)
            upper += jnp.dot(rows, wu[q * COLS : (q + 1) * COLS, :], preferred_element_type=F32)
        hid[c, tp] = (gate / (1.0 + jnp.exp(-gate)) * upper).astype(BF16)
        mine = hid.at[c, tp]
        y_copy(mine, mine, 12, rh0p.at[c], up).start()
        y_copy(mine, mine, 13, rh0m.at[c], down).start()

    def hidden_on(c):
        y_copy(hid.at[c, down], hid.at[c, down], 12, rh0p.at[c], up).wait_recv()
        half = hid.at[c, down, pl.ds(0, HALF)]
        y_copy(half, half, 14, rhfp.at[c], up).start()
        y_copy(hid.at[c, up], hid.at[c, up], 13, rh0m.at[c], down).wait_recv()
        half = hid.at[c, up, pl.ds(HALF, HALF)]
        y_copy(half, half, 15, rhfm.at[c], down).start()

    def results_out(c):
        at = plane(c) * PER_Z

        @pl.when(c == 0)
        def _():
            whole = wdq.at[0]
            half = wdq.at[0, pl.ds(0, 128)]
            y_copy(whole, whole, 0, rwd.at[0], up).wait_recv()
            y_copy(whole, whole, 1, rwd.at[1], down).wait_recv()
            y_copy(half, half, 4, rwd.at[4], up).wait_recv()
            y_copy(half, half, 5, rwd.at[5], down).wait_recv()

        half = hid.at[c, across, pl.ds(0, HALF)]
        y_copy(half, half, 14, rhfp.at[c], up).wait_recv()
        half = hid.at[c, across, pl.ds(HALF, HALF)]
        y_copy(half, half, 15, rhfm.at[c], down).wait_recv()
        sums = jnp.zeros((CHUNK, COLS), F32)
        for q in range(N_TP):
            term = jnp.dot(hid[c, q], wdq[q], preferred_element_type=F32)
            sums += term.astype(BF16).astype(F32)
        res[c] = sums.astype(BF16).reshape(PER_Z, CAP, COLS)

        def put(j):
            remote(
                res.at[c, j], ret.at[ep], send.at[16], rret.at[c], {"ep": at + j}
            ).start()

        @pl.when(c != 0)
        def _():
            put(xc)

        @pl.when(c == 0)
        def _():
            ret[pl.ds(ep, 1)] = res[c, pl.ds(xc, 1)]

        @pl.loop(1, PER_Z)
        def _(j):
            put((xc + j) % PER_Z)

    def combine(c):
        far = ((z + chunk_offset(c)) % N_Z) * PER_Z
        whole = ret.at[pl.ds(far, PER_Z)]
        less = ret.at[pl.ds(0, PER_Z - 1)]

        @pl.when(c == 0)
        def _():
            remote(less, less, send.at[16], rret.at[c], {"tp": up}).wait_recv()

        @pl.when(c != 0)
        def _():
            remote(whole, whole, send.at[16], rret.at[c], {"tp": up}).wait_recv()

        ids = (lax.broadcasted_iota(jnp.int32, (128, CHUNK), 1) + far * CAP).astype(F32)
        back = ret[pl.ds(far, PER_Z)].reshape(CHUNK, COLS)

        for i in range(4):
            sel = slice(i * 128, (i + 1) * 128)
            sums = moe_ref[sel, :]
            for k in range(2):
                pick = (ids == columned[sel, k : k + 1]).astype(BF16)
                got_rows = jnp.dot(pick, back, preferred_element_type=F32)
                sums += got_rows * columned[sel, 2 + k : 3 + k]
            moe_ref[sel, :] = sums

    def relay(c):
        y_copy(relay_p, relay_p, 2, rwd.at[2], up).wait_recv()
        y_copy(relay_p, wdq.at[down, pl.ds(0, 128)], 4, rwd.at[4], up).start()
        y_copy(relay_m, relay_m, 3, rwd.at[3], down).wait_recv()
        y_copy(relay_m, wdq.at[up, pl.ds(128, 128)], 5, rwd.at[5], down).start()

    def attend(c):
        at = latent_plane(c)
        four = lat.at[1 - core, at]
        remote(four, four, send.at[18], rld.at[c], {"tp": up}).wait_recv()
        turned = lat[:, at, :, 128:160, :].reshape(256, 256)
        keys = []
        scores = []
        for g in range(4):
            keys.append(lat[:, at, :, g * 32 : (g + 1) * 32, :].reshape(256, 256))
            s = lax.dot_general(query[...], keys[g], NT, preferred_element_type=F32)
            s += lax.dot_general(qrot[g], turned, NT, preferred_element_type=F32)
            scores.append(s * (SCORE_SCALE * LOG2E))
        peak = jnp.maximum(
            jnp.maximum(scores[0], scores[1]), jnp.maximum(scores[2], scores[3])
        )
        new_top = jnp.maximum(top[...], jnp.max(peak, axis=1, keepdims=True))
        fade = jnp.exp2(top[...] - new_top)
        weighed = acc[...] * fade
        sums = jnp.zeros((256, 256), F32)
        for g in range(4):
            weights = jnp.exp2(scores[g] - new_top)
            sums += weights
            weighed += jnp.dot(weights.astype(BF16), keys[g], preferred_element_type=F32)
        total[...] = total[...] * fade + jnp.sum(sums, axis=1, keepdims=True)
        acc[...] = weighed
        top[...] = new_top

    def mix_copy(i):
        other = (tp + i) % N_TP
        return remote(mix.at[other], got.at[i], send.at[18 + i], rmix.at[i], {"tp": other})

    def project(c):
        mean = (acc[...] / total[...]).astype(BF16)
        heads = []
        for h in range(2):
            sel = slice(h * 128, (h + 1) * 128)
            heads.append(
                jnp.dot(mean[sel], wv[:, sel], preferred_element_type=F32).astype(BF16)
            )
        heads = jnp.concatenate(heads, axis=1)
        for q in range(4):
            sel = slice(q * 512, (q + 1) * 512)
            term = jnp.dot(heads, wo[:, sel], preferred_element_type=F32)
            mix[:, :, sel] = term.astype(BF16).reshape(N_TP, 32, 512)
        for i in range(1, N_TP):
            mix_copy(i).start()

    def twice(stage, start):
        def both(c):
            stage(start + 2 * c)
            stage(start + 1 + 2 * c)

        both.__name__ = stage.__name__
        return both

    def after(stage, start):
        def later(c):
            stage(start + c)

        later.__name__ = stage.__name__
        return later

    plan = (
        (0, 7, after(tokens_in, 1)),
        (0, 1, relay),
        (1, 7, after(tokens_on, 1)),
        (1, 8, hidden_units),
        (2, 8, hidden_on),
        (3, 8, results_out),
        (0, 2, after(latents_x, 1)),
        (3, 2, twice(latents_x, 3)),
        (5, 1, after(latents_x, 7)),
        (0, 3, latents_on),
        (4, 2, twice(latents_on, 3)),
        (6, 1, after(latents_on, 7)),
        (1, 3, latents_core),
        (5, 2, twice(latents_core, 3)),
        (7, 1, after(latents_core, 7)),
        (2, 3, attend),
        (6, 2, twice(attend, 3)),
        (9, 1, after(attend, 7)),
        (9, 1, project),
        (6, 2, combine),
        (10, 6, after(combine, 2)),
    )

    @pl.loop(0, 16)
    def _(i):
        for lag, count, stage in plan:

            @pl.when((i >= lag) & (i < lag + count))
            def _(stage=stage, lag=lag):
                stage(i - lag)

    sums = mix[tp].astype(F32)
    for i in range(1, N_TP):
        mix_copy(i).wait()
        sums = sums + got[i].astype(F32)
    mixed_ref[...] = sums

    def sent(ref, which):
        remote(ref, ref, send.at[which], ra2a.at[0], {"tp": up}).wait_send()

    for which in (0, 1):
        sent(wdq.at[0], which)
    for which in (2, 3, 4, 5):
        sent(relay_p, which)
    sent(outg.at[0, pl.ds(0, 56)], 6)
    sent(outg.at[:, pl.ds(0, 7)], 23)
    sent(lat.at[0, pl.ds(0, 7), 0], 7)
    for which in (8, 9):
        sent(arr.at[0, pl.ds(0, 56)], which)
    for which in (10, 11):
        sent(arr.at[0, pl.ds(0, 28)], which)
    for which in (12, 13):
        sent(hid.at[:, 0], which)
    for which in (14, 15):
        sent(hid.at[:, 0, pl.ds(0, HALF)], which)
    sent(ret.at[pl.ds(0, N_EP - 1)], 16)
    sent(lat.at[0, :, pl.ds(0, 2)], 17)
    sent(lat.at[0, :, 0], 22)
    sent(lat.at[0], 18)


def finish_kernel(moe_ref, mixed_ref, moe_out, mixed_out):
    moe_out[...] = moe_ref[...].astype(BF16)
    mixed_out[...] = mixed_ref[...].astype(BF16)


VM = pl.BlockSpec(memory_space=pltpu.VMEM)
ANY = pl.BlockSpec(memory_space=pl.ANY)


def struct(shape, dtype=BF16):
    return jax.ShapeDtypeStruct(shape, dtype)


def body(
    query_latent, key_latent, rope_key, query_gain, key_gain, w_query, w_query_rope, w_key,
    w_value, w_out, tokens_b, ffn_gain, route_expert, route_weight, w_gate, w_up, w_down,
):
    rows_np, cols_np = rotary_consts()
    rows = jnp.asarray(rows_np)
    cols = jnp.asarray(cols_np)
    dma = pltpu.SemaphoreType.DMA

    moe, mixed = pl.pallas_call(
        main_kernel,
        out_shape=(
            struct((512, COLS), F32),
            struct((32, 2048), F32),
        ),
        in_specs=[ANY] * 19,
        out_specs=(VM, VM),
        scratch_shapes=[
            pltpu.VMEM(shape, dtype)
            for shape, dtype in (
                ((1, 2048), F32),
                ((2, 512), jnp.int32),
                ((2, 512), F32),
                ((128, 256), BF16),
                ((64, 128), BF16),
                ((1, 256), F32),
                ((128, 512), BF16),
                ((1, 512), F32),
                ((4, 128), F32),
                ((2, 64, 128), F32),
                ((512, 2048), BF16),
                ((2048, 256), BF16),
                ((2048, 256), BF16),
                ((512, 256), BF16),
                ((512, 128), BF16),
                ((256, 256), BF16),
                ((256, 256), BF16),
                ((256, 2048), BF16),
                ((N_TP, 256, COLS), BF16),
                ((128, COLS), BF16),
                ((128, COLS), BF16),
                ((512, 2048), BF16),
                ((N_TP, N_EP, CAP, COLS), BF16),
                ((N_TP, N_EP, CAP, COLS), BF16),
                ((N_Z, N_TP, CHUNK, 256), BF16),
                ((N_Z, PER_Z, CAP, COLS), BF16),
                ((N_EP, CAP, COLS), BF16),
                ((512, 128), F32),
                ((2, N_Z, 4, 160, 256), BF16),
                ((256, 256), BF16),
                ((4, 256, 256), BF16),
                ((256, 1), F32),
                ((256, 1), F32),
                ((256, 256), F32),
                ((N_TP, 32, 2048), BF16),
                ((N_TP, 32, 2048), BF16),
            )
        ]
        + [dma((19,)), dma((24,)), dma((6,)), dma((N_TP,))]
        + [dma((N_Z,))] * 16,
        compiler_params=pltpu.CompilerParams(
            collective_id=0, has_side_effects=True, vmem_limit_bytes=VMEM_LIMIT
        ),
        name="exchange",
    )(
        ffn_gain.reshape(1, -1), route_expert.T, route_weight.T, key_latent, rope_key.T, key_gain.reshape(1, -1),
        query_latent, query_gain.reshape(1, -1), rows, cols,
        tokens_b, w_gate[0], w_up[0], w_down[0], w_query, w_query_rope, w_key, w_value, w_out,
    )

    moe_out, mixer_out = pl.pallas_call(
        finish_kernel,
        out_shape=(struct((512, COLS)), struct((32, 2048))),
        in_specs=[VM] * 2,
        out_specs=(VM, VM),
        compiler_params=pltpu.CompilerParams(vmem_limit_bytes=VMEM_LIMIT),
        name="finish",
    )(moe, mixed)

    return (mixer_out, moe_out)


def solution(mesh):
    in_specs = (
        P("ep", None),
        P("ep", None),
        P("ep", None),
        P(),
        P(),
        P(None, "tp"),
        P(None, "tp"),
        P(None, "tp"),
        P(None, "tp"),
        P("tp", None),
        P("ep", None),
        P(),
        P("ep", None),
        P("ep", None),
        P("ep", None, "tp"),
        P("ep", None, "tp"),
        P("ep", "tp", None),
    )
    out_specs = (P(("ep", "tp"), None), P("ep", "tp"))
    return jax.shard_map(body, mesh=mesh, in_specs=in_specs, out_specs=out_specs, check_vma=False)
```

```python
import math

import jax
import jax.numpy as jnp
import numpy as np
from jax import lax
from jax.experimental import pallas as pl
from jax.experimental.pallas import tpu as pltpu
from jax.sharding import PartitionSpec as P

NOPE = 128
ROPE = 64
GRID_W = 64
epsilon = 1e-06
rotary_base = 10000.0
LOG2E = 1.4426950408889634
SCORE_SCALE = (NOPE + ROPE) ** (-0.5)

F32 = jnp.float32
BF16 = jnp.bfloat16
MESH = pl.DeviceIdType.MESH

N_EP = 64
N_TP = 4
PER_Z = 8
N_Z = 8
CAP = 16
COLS = 512
CHUNK = PER_Z * CAP
HALF = CHUNK // 2
VMEM_LIMIT = 62 * 1024 * 1024


def rotary_consts():
    inverse = np.float32(rotary_base) ** (-np.arange(0, 32, 2, dtype=np.float32) / np.float32(32))
    inverse = inverse.astype(np.float32)
    entry = np.arange(128) % ROPE
    pair = entry // 2
    row_lane = pair < 16
    freq = inverse[pair % 16]
    row_angle = (np.arange(128, dtype=np.float32)[:, None] * freq[None, :]).astype(np.float32)
    col_angle = (np.arange(64, dtype=np.float32)[:, None] * freq[None, :]).astype(np.float32)

    def both(angle, keep):
        wide = angle.astype(np.float64)
        return [np.where(keep, fn(wide), 0.0).astype(np.float32) for fn in (np.cos, np.sin)]

    row_cos, row_sin = both(row_angle, row_lane[None, :])
    col_cos, col_sin = both(col_angle, ~row_lane[None, :])
    rows = np.stack([row_cos.reshape(64, 2, 128), row_sin.reshape(64, 2, 128)], axis=1)
    rows = rows.reshape(64, 4, 128)
    cols = np.stack([col_cos, col_sin], axis=0)
    return rows, cols


def cos_sin(rows_ref, cols_ref):
    rows = rows_ref[...]
    cos = jnp.concatenate([rows[0:1] + cols_ref[0], rows[1:2] + cols_ref[0]], axis=0)
    sin = jnp.concatenate([rows[2:3] + cols_ref[1], rows[3:4] + cols_ref[1]], axis=0)
    return cos, sin


def turn(x, cos, sin):
    lane = lax.broadcasted_iota(jnp.int32, x.shape, 1)
    swapped = jnp.where(lane % 2 == 0, -pltpu.roll(x, 127, 1), pltpu.roll(x, 1, 1))
    return x * cos + swapped * sin


def rms(x, gain):
    wide = x.astype(F32)
    normed = wide * lax.rsqrt(jnp.mean(wide * wide, axis=-1, keepdims=True) + epsilon)
    return (normed * gain).astype(BF16)


NT = (((1,), (1,)), ((), ()))


ORDER_BENDS = ((1, 7), (2, 6), (-3, 5), (1, 3), (-6, 2), (5, 1))


def chunk_offset(c):
    bend = sum(k * ((c + start) // 8) for k, start in ORDER_BENDS)
    return c + bend


def all_columns(c):
    return c == 0


def latent_offset(a):
    return (a % 2) * ((a + 1) // 2) + (1 - a % 2) * ((8 - a // 2) % 8)


def remote(src, dst, send, recv, where):
    return pltpu.make_async_remote_copy(
        src_ref=src, dst_ref=dst, send_sem=send, recv_sem=recv, device_id=where, device_id_type=MESH
    )


def main_kernel(
    gain_hbm, route_hbm, weight_hbm, klat_hbm, rope_hbm, kgain_hbm, qlat_hbm, qgain_hbm, rows_hbm, cols_hbm,
    tok_hbm, wg_hbm, wu_hbm, wd_hbm, wq_hbm, wqr_hbm, wk_hbm, wv_hbm, wo_hbm,
    moe_ref, mixed_ref,
    gain_ref, route_ref, weight_ref, klat_ref, rope_ref, kgain_ref, qlat_ref, qgain_ref, rows_ref, cols_ref,
    tok, wg, wu, wq, wqr, wk, wv, wo, wdq, relay_p, relay_m,
    normed, outg, arr, hid, res, ret, columned, weighed_rows, lat, query, qrot, top, total, acc, mix, got,
    wsem, send, rwd, rmix, ra2a, ry0p, ry0m, rfwp, rfwm, rh0p, rh0m, rhfp, rhfm, rret, rlz, rlxp, rlxm, rlfp, rlfm, rld,
):
    ep = lax.axis_index("ep")
    tp = lax.axis_index("tp")
    z = ep // PER_Z
    xc = ep % PER_Z
    x = xc // 2
    core = xc % 2
    up = (tp + 1) % N_TP
    down = (tp + N_TP - 1) % N_TP
    across = (tp + 2) % N_TP

    barrier = pltpu.get_barrier_semaphore()

    @pl.loop(1, N_EP)
    def _(i):
        pl.semaphore_signal(
            barrier, inc=1, device_id={"ep": (ep + i) % N_EP}, device_id_type=MESH
        )

    for other in (up, down, across):
        pl.semaphore_signal(barrier, inc=1, device_id={"tp": other}, device_id_type=MESH)

    def columns(which):
        return pl.ds(pl.multiple_of(which * COLS, COLS), COLS)

    pairs = (
        (klat_hbm, klat_ref), (kgain_hbm, kgain_ref), (rope_hbm, rope_ref),
        (rows_hbm.at[ep], rows_ref), (cols_hbm, cols_ref), (route_hbm, route_ref),
        (gain_hbm, gain_ref), (tok_hbm, tok), (weight_hbm, weight_ref), (qlat_hbm, qlat_ref),
        (qgain_hbm, qgain_ref), (wd_hbm.at[:, columns(tp)], wdq.at[tp]), (wg_hbm, wg), (wu_hbm, wu),
        (wq_hbm, wq), (wqr_hbm, wqr), (wk_hbm, wk), (wv_hbm, wv), (wo_hbm, wo),
    )
    loads = [pltpu.make_async_copy(src, dst, wsem.at[i]) for i, (src, dst) in enumerate(pairs)]
    for load in loads:
        load.start()

    for load in loads[0:6]:
        load.wait()

    cos, sin = cos_sin(rows_ref, cols_ref)
    lat[core, z, x, 0:128, :] = rms(klat_ref[...], kgain_ref[...])
    rope = rope_ref[...].astype(F32)
    rope = jnp.concatenate([rope, rope], axis=0).T
    turned = turn(rope, cos, sin)
    low = lax.broadcasted_iota(jnp.int32, (32, 128), 1) < ROPE
    left = jnp.where(low, turned[0:32], turned[32:64])
    right = jnp.where(low, turned[64:96], turned[96:128])
    lat[core, z, x, 128:160, :] = jnp.concatenate([left, right], axis=1).astype(BF16)

    route = route_ref[...]
    first = route[0:1, :]
    second = route[1:2, :]
    ids = lax.broadcasted_iota(jnp.int32, (N_EP, 512), 0)
    hit0 = (ids == first).astype(F32)
    hit1 = (ids == second).astype(F32)
    before = lax.broadcasted_iota(jnp.int32, (512, 512), 0) < lax.broadcasted_iota(
        jnp.int32, (512, 512), 1
    )
    earlier = jnp.dot((hit0 + hit1).astype(BF16), before.astype(BF16), preferred_element_type=F32)
    slot0 = jnp.sum(hit0 * earlier, axis=0, keepdims=True).astype(jnp.int32)
    slot1 = jnp.sum(hit1 * earlier, axis=0, keepdims=True).astype(jnp.int32)
    target0 = first * CAP + slot0
    target1 = second * CAP + slot1

    pl.semaphore_wait(barrier, N_EP - 1 + 3)

    def y_copy(src, dst, send_at, recv, where):
        return remote(src, dst, send.at[send_at], recv, {"tp": where})

    y_copy(wd_hbm.at[:, columns(up)], wdq.at[tp], 0, rwd.at[0], up).start()
    y_copy(wd_hbm.at[:, columns(down)], wdq.at[tp], 1, rwd.at[1], down).start()
    y_copy(wd_hbm.at[pl.ds(0, 128), columns(across)], relay_p, 2, rwd.at[2], up).start()
    y_copy(wd_hbm.at[pl.ds(128, 128), columns(across)], relay_m, 3, rwd.at[3], down).start()

    def latent_plane(a):
        return (z + N_Z - latent_offset(a)) % N_Z

    def ep_at(z_at, x_at):
        return ((z_at + N_Z) % N_Z) * PER_Z + ((x_at + 4) % 4) * 2 + core

    def latents_x(a):
        block = lat.at[core, latent_plane(a), x]

        def along_z(step, which):
            remote(block, block, send.at[7], rlz.at[which], {"ep": ep_at(z + step, x)}).start()

        @pl.when(a != 0)
        def _():
            remote(block, block, send.at[7], rlz.at[a], {"tp": up}).wait_recv()

        @pl.when(a == 0)
        def _():
            along_z(1, 1)
            along_z(-1, 2)

        @pl.when((a % 2 == 1) & (a < 7))
        def _():
            along_z(1, a + 2)

        @pl.when((a % 2 == 0) & (a > 0) & (a < 6))
        def _():
            along_z(-1, a + 2)

        remote(block, block, send.at[17], rlxp.at[a], {"ep": ep_at(z, x + 1)}).start()
        remote(block, block, send.at[17], rlxm.at[a], {"ep": ep_at(z, x - 1)}).start()

    def latents_on(a):
        at = latent_plane(a)
        below = lat.at[core, at, (x + 3) % 4]
        remote(below, below, send.at[17], rlxp.at[a], {"tp": up}).wait_recv()
        half = lat.at[core, at, (x + 3) % 4, pl.ds(0, 80)]
        remote(half, half, send.at[22], rlfp.at[a], {"ep": ep_at(z, x + 1)}).start()
        above = lat.at[core, at, (x + 1) % 4]
        remote(above, above, send.at[17], rlxm.at[a], {"tp": up}).wait_recv()
        half = lat.at[core, at, (x + 1) % 4, pl.ds(80, 80)]
        remote(half, half, send.at[22], rlfm.at[a], {"ep": ep_at(z, x - 1)}).start()

    def latents_core(a):
        at = latent_plane(a)
        half = lat.at[core, at, (x + 2) % 4, pl.ds(0, 80)]
        remote(half, half, send.at[22], rlfp.at[a], {"tp": up}).wait_recv()
        half = lat.at[core, at, (x + 2) % 4, pl.ds(80, 80)]
        remote(half, half, send.at[22], rlfm.at[a], {"tp": up}).wait_recv()
        four = lat.at[core, at]
        remote(four, four, send.at[18], rld.at[a], {"ep": z * PER_Z + x * 2 + (1 - core)}).start()

    latents_x(0)

    loads[6].wait()
    loads[7].wait()

    @pl.loop(0, 8)
    def _(i):
        sel = pl.ds(pl.multiple_of(i * 64, 64), 64)
        wide = tok[sel, :].astype(F32)
        scale = lax.rsqrt(jnp.mean(wide * wide, axis=-1, keepdims=True) + epsilon)
        normed[sel, :] = (wide * scale * gain_ref[...]).astype(BF16)

    def rows_out(c):
        zd = (z + chunk_offset(c)) % N_Z
        far = zd * PER_Z
        ids = lax.broadcasted_iota(jnp.int32, (CHUNK, 512), 0) + zd * CHUNK
        pick = ((ids == target0) | (ids == target1)).astype(BF16)

        def take(q):
            rows = jnp.dot(pick, normed[:, columns(q)], preferred_element_type=F32).astype(BF16)
            outg[q, pl.ds(far, PER_Z)] = rows.reshape(PER_Z, CAP, COLS)

        @pl.when(all_columns(c))
        def _():
            for q in range(N_TP):
                take(q)

            def put(other):
                remote(
                    outg.at[:, other], arr.at[:, ep], send.at[23], ra2a.at[c], {"ep": other}
                ).start()

            @pl.loop(1, PER_Z)
            def _(j):
                put(far + (xc + j) % PER_Z)

        @pl.when(jnp.logical_not(all_columns(c)))
        def _():
            take(tp)

            @pl.loop(0, PER_Z)
            def _(j):
                other = far + (xc + j) % PER_Z
                remote(
                    outg.at[tp, other], arr.at[tp, ep], send.at[6], ra2a.at[c], {"ep": other}
                ).start()

    @pl.loop(0, N_Z)
    def _(i):
        rows_out(i + (7 - i) // 7 - (8 - i) // 7 + (8 - i) // 8)

    arr[:, pl.ds(ep, 1)] = outg[:, pl.ds(ep, 1)]

    for load in loads[8:]:
        load.wait()

    qn = rms(qlat_ref[...], qgain_ref[...])
    nope = jnp.dot(qn, wq[...], preferred_element_type=F32).astype(BF16)
    for h in range(2):
        sel = slice(h * 128, (h + 1) * 128)
        query[sel, :] = lax.dot_general(
            nope[:, sel], wk[:, sel], NT, preferred_element_type=F32
        ).astype(BF16)
    rot = turn(jnp.dot(qn, wqr[...], preferred_element_type=F32), cos, sin)
    low = lax.broadcasted_iota(jnp.int32, (128, 128), 1) < ROPE
    rolled = pltpu.roll(rot, ROPE, 1)
    near = jnp.concatenate([jnp.where(low, rot, 0.0), jnp.where(low, rolled, 0.0)], axis=0)
    far = jnp.concatenate([jnp.where(low, 0.0, rolled), jnp.where(low, 0.0, rot)], axis=0)
    near = near.astype(BF16)
    far = far.astype(BF16)
    none = jnp.zeros((256, 128), BF16)
    for g, pair in enumerate(((near, none), (far, none), (none, near), (none, far))):
        qrot[g] = jnp.concatenate(pair, axis=1)
    columned[...] = jnp.concatenate(
        [target0.astype(F32), target1.astype(F32), weight_ref[...], jnp.zeros((124, 512), F32)], axis=0
    ).T
    weighed_rows[...] = jnp.zeros((512, COLS), F32)
    top[...] = jnp.full((256, 1), -1e30, F32)
    total[...] = jnp.zeros((256, 1), F32)
    acc[...] = jnp.zeros((256, 256), F32)

    def plane(c):
        return (z + N_Z - chunk_offset(c)) % N_Z

    def tokens_in(c):
        at = plane(c) * PER_Z
        whole = arr.at[tp, pl.ds(at, PER_Z)]
        remote(whole, whole, send.at[6], ra2a.at[c], {"tp": up}).wait_recv()
        y_copy(whole, whole, 8, ry0p.at[c], up).start()
        y_copy(whole, whole, 9, ry0m.at[c], down).start()

    def tokens_on(c):
        at = plane(c) * PER_Z
        below = arr.at[down, pl.ds(at, PER_Z)]
        above = arr.at[up, pl.ds(at, PER_Z)]
        y_copy(below, below, 8, ry0p.at[c], up).wait_recv()
        half = arr.at[down, pl.ds(at, PER_Z // 2)]
        y_copy(half, half, 10, rfwp.at[c], up).start()
        y_copy(above, above, 9, ry0m.at[c], down).wait_recv()
        half = arr.at[up, pl.ds(at + PER_Z // 2, PER_Z // 2)]
        y_copy(half, half, 11, rfwm.at[c], down).start()

    def hidden_units(c):
        at = plane(c) * PER_Z

        @pl.when(c == 0)
        def _():
            less = arr.at[:, pl.ds(0, PER_Z - 1)]
            remote(less, less, send.at[23], ra2a.at[c], {"tp": up}).wait_recv()

        @pl.when(jnp.logical_not(all_columns(c)))
        def _():
            half = arr.at[across, pl.ds(at, PER_Z // 2)]
            y_copy(half, half, 10, rfwp.at[c], up).wait_recv()
            half = arr.at[across, pl.ds(at + PER_Z // 2, PER_Z // 2)]
            y_copy(half, half, 11, rfwm.at[c], down).wait_recv()

        gate = jnp.zeros((CHUNK, 256), F32)
        upper = jnp.zeros((CHUNK, 256), F32)
        for q in range(N_TP):
            rows = arr[q, pl.ds(at, PER_Z)].reshape(CHUNK, COLS)
            gate += jnp.dot(rows, wg[q * COLS : (q + 1) * COLS, :], preferred_element_type=F32)
            upper += jnp.dot(rows, wu[q * COLS : (q + 1) * COLS, :], preferred_element_type=F32)
        hid[c, tp] = (gate / (1.0 + jnp.exp(-gate)) * upper).astype(BF16)
        mine = hid.at[c, tp]
        y_copy(mine, mine, 12, rh0p.at[c], up).start()
        y_copy(mine, mine, 13, rh0m.at[c], down).start()

    def hidden_on(c):
        y_copy(hid.at[c, down], hid.at[c, down], 12, rh0p.at[c], up).wait_recv()
        half = hid.at[c, down, pl.ds(0, HALF)]
        y_copy(half, half, 14, rhfp.at[c], up).start()
        y_copy(hid.at[c, up], hid.at[c, up], 13, rh0m.at[c], down).wait_recv()
        half = hid.at[c, up, pl.ds(HALF, HALF)]
        y_copy(half, half, 15, rhfm.at[c], down).start()

    def results_out(c):
        at = plane(c) * PER_Z

        @pl.when(c == 0)
        def _():
            whole = wdq.at[0]
            half = wdq.at[0, pl.ds(0, 128)]
            y_copy(whole, whole, 0, rwd.at[0], up).wait_recv()
            y_copy(whole, whole, 1, rwd.at[1], down).wait_recv()
            y_copy(half, half, 4, rwd.at[4], up).wait_recv()
            y_copy(half, half, 5, rwd.at[5], down).wait_recv()

        half = hid.at[c, across, pl.ds(0, HALF)]
        y_copy(half, half, 14, rhfp.at[c], up).wait_recv()
        half = hid.at[c, across, pl.ds(HALF, HALF)]
        y_copy(half, half, 15, rhfm.at[c], down).wait_recv()
        sums = jnp.zeros((CHUNK, COLS), F32)
        for q in range(N_TP):
            term = jnp.dot(hid[c, q], wdq[q], preferred_element_type=F32)
            sums += term.astype(BF16).astype(F32)
        res[c] = sums.astype(BF16).reshape(PER_Z, CAP, COLS)

        def put(j):
            remote(
                res.at[c, j], ret.at[ep], send.at[16], rret.at[c], {"ep": at + j}
            ).start()

        @pl.when(c != 0)
        def _():
            put(xc)

        @pl.when(c == 0)
        def _():
            ret[pl.ds(ep, 1)] = res[c, pl.ds(xc, 1)]

        @pl.loop(1, PER_Z)
        def _(j):
            put((xc + j) % PER_Z)

    def combine(c):
        far = ((z + chunk_offset(c)) % N_Z) * PER_Z
        whole = ret.at[pl.ds(far, PER_Z)]
        less = ret.at[pl.ds(0, PER_Z - 1)]

        @pl.when(c == 0)
        def _():
            remote(less, less, send.at[16], rret.at[c], {"tp": up}).wait_recv()

        @pl.when(c != 0)
        def _():
            remote(whole, whole, send.at[16], rret.at[c], {"tp": up}).wait_recv()

        ids = (lax.broadcasted_iota(jnp.int32, (128, CHUNK), 1) + far * CAP).astype(F32)
        back = ret[pl.ds(far, PER_Z)].reshape(CHUNK, COLS)

        for i in range(4):
            sel = slice(i * 128, (i + 1) * 128)
            sums = weighed_rows[sel, :]
            for k in range(2):
                pick = (ids == columned[sel, k : k + 1]).astype(BF16)
                got_rows = jnp.dot(pick, back, preferred_element_type=F32)
                sums += got_rows * columned[sel, 2 + k : 3 + k]
            weighed_rows[sel, :] = sums

    def relay(c):
        y_copy(relay_p, relay_p, 2, rwd.at[2], up).wait_recv()
        y_copy(relay_p, wdq.at[down, pl.ds(0, 128)], 4, rwd.at[4], up).start()
        y_copy(relay_m, relay_m, 3, rwd.at[3], down).wait_recv()
        y_copy(relay_m, wdq.at[up, pl.ds(128, 128)], 5, rwd.at[5], down).start()

    def attend(c):
        at = latent_plane(c)
        four = lat.at[1 - core, at]
        remote(four, four, send.at[18], rld.at[c], {"tp": up}).wait_recv()
        turned = lat[:, at, :, 128:160, :].reshape(256, 256)
        keys = []
        scores = []
        for g in range(4):
            keys.append(lat[:, at, :, g * 32 : (g + 1) * 32, :].reshape(256, 256))
            s = lax.dot_general(query[...], keys[g], NT, preferred_element_type=F32)
            s += lax.dot_general(qrot[g], turned, NT, preferred_element_type=F32)
            scores.append(s * (SCORE_SCALE * LOG2E))
        peak = jnp.maximum(
            jnp.maximum(scores[0], scores[1]), jnp.maximum(scores[2], scores[3])
        )
        new_top = jnp.maximum(top[...], jnp.max(peak, axis=1, keepdims=True))
        fade = jnp.exp2(top[...] - new_top)
        weighed = acc[...] * fade
        sums = jnp.zeros((256, 256), F32)
        for g in range(4):
            weights = jnp.exp2(scores[g] - new_top)
            sums += weights
            weighed += jnp.dot(weights.astype(BF16), keys[g], preferred_element_type=F32)
        total[...] = total[...] * fade + jnp.sum(sums, axis=1, keepdims=True)
        acc[...] = weighed
        top[...] = new_top

    def mix_copy(i):
        other = (tp + i) % N_TP
        return remote(mix.at[other], got.at[i], send.at[18 + i], rmix.at[i], {"tp": other})

    def project(c):
        mean = (acc[...] / total[...]).astype(BF16)
        heads = []
        for h in range(2):
            sel = slice(h * 128, (h + 1) * 128)
            heads.append(
                jnp.dot(mean[sel], wv[:, sel], preferred_element_type=F32).astype(BF16)
            )
        heads = jnp.concatenate(heads, axis=1)
        for q in range(4):
            sel = slice(q * 512, (q + 1) * 512)
            term = jnp.dot(heads, wo[:, sel], preferred_element_type=F32)
            mix[:, :, sel] = term.astype(BF16).reshape(N_TP, 32, 512)
        for i in range(1, N_TP):
            mix_copy(i).start()

    def twice(stage, start):
        def both(c):
            stage(start + 2 * c)
            stage(start + 1 + 2 * c)

        both.__name__ = stage.__name__
        return both

    def after(stage, start):
        def later(c):
            stage(start + c)

        later.__name__ = stage.__name__
        return later

    plan = (
        (0, 7, after(tokens_in, 1)),
        (0, 1, relay),
        (1, 7, after(tokens_on, 1)),
        (1, 8, hidden_units),
        (2, 8, hidden_on),
        (3, 8, results_out),
        (0, 2, after(latents_x, 1)),
        (3, 2, twice(latents_x, 3)),
        (5, 1, after(latents_x, 7)),
        (0, 3, latents_on),
        (4, 2, twice(latents_on, 3)),
        (6, 1, after(latents_on, 7)),
        (1, 3, latents_core),
        (5, 2, twice(latents_core, 3)),
        (7, 1, after(latents_core, 7)),
        (2, 3, attend),
        (6, 2, twice(attend, 3)),
        (9, 1, after(attend, 7)),
        (9, 1, project),
        (6, 2, combine),
        (10, 6, after(combine, 2)),
    )

    @pl.loop(0, 16)
    def _(i):
        for lag, count, stage in plan:

            @pl.when((i >= lag) & (i < lag + count))
            def _(stage=stage, lag=lag):
                stage(i - lag)

    sums = mix[tp].astype(F32)
    for i in range(1, N_TP):
        mix_copy(i).wait()
        sums = sums + got[i].astype(F32)
    mixed_ref[...] = sums.astype(BF16)

    moe_ref[...] = weighed_rows[...].astype(BF16)

    def sent(ref, which):
        remote(ref, ref, send.at[which], ra2a.at[0], {"tp": up}).wait_send()

    for which in (0, 1):
        sent(wdq.at[0], which)
    for which in (2, 3, 4, 5):
        sent(relay_p, which)
    sent(outg.at[0, pl.ds(0, 56)], 6)
    sent(outg.at[:, pl.ds(0, 7)], 23)
    sent(lat.at[0, pl.ds(0, 7), 0], 7)
    for which in (8, 9):
        sent(arr.at[0, pl.ds(0, 56)], which)
    for which in (10, 11):
        sent(arr.at[0, pl.ds(0, 28)], which)
    for which in (12, 13):
        sent(hid.at[:, 0], which)
    for which in (14, 15):
        sent(hid.at[:, 0, pl.ds(0, HALF)], which)
    sent(ret.at[pl.ds(0, N_EP - 1)], 16)
    sent(lat.at[0, :, pl.ds(0, 2)], 17)
    sent(lat.at[0, :, 0], 22)
    sent(lat.at[0], 18)


def finish_kernel(moe_ref, mixed_ref, moe_out, mixed_out):
    moe_out[...] = moe_ref[...]
    mixed_out[...] = mixed_ref[...]


VM = pl.BlockSpec(memory_space=pltpu.VMEM)
ANY = pl.BlockSpec(memory_space=pl.ANY)


def struct(shape, dtype=BF16):
    return jax.ShapeDtypeStruct(shape, dtype)


def body(
    query_latent, key_latent, rope_key, query_gain, key_gain, w_query, w_query_rope, w_key,
    w_value, w_out, tokens_b, ffn_gain, route_expert, route_weight, w_gate, w_up, w_down,
):
    rows_np, cols_np = rotary_consts()
    rows = jnp.asarray(rows_np)
    cols = jnp.asarray(cols_np)
    dma = pltpu.SemaphoreType.DMA

    moe, mixed = pl.pallas_call(
        main_kernel,
        out_shape=(
            struct((512, COLS)),
            struct((32, 2048)),
        ),
        in_specs=[ANY] * 19,
        out_specs=(VM, VM),
        scratch_shapes=[
            pltpu.VMEM(shape, dtype)
            for shape, dtype in (
                ((1, 2048), F32),
                ((2, 512), jnp.int32),
                ((2, 512), F32),
                ((128, 256), BF16),
                ((64, 128), BF16),
                ((1, 256), F32),
                ((128, 512), BF16),
                ((1, 512), F32),
                ((4, 128), F32),
                ((2, 64, 128), F32),
                ((512, 2048), BF16),
                ((2048, 256), BF16),
                ((2048, 256), BF16),
                ((512, 256), BF16),
                ((512, 128), BF16),
                ((256, 256), BF16),
                ((256, 256), BF16),
                ((256, 2048), BF16),
                ((N_TP, 256, COLS), BF16),
                ((128, COLS), BF16),
                ((128, COLS), BF16),
                ((512, 2048), BF16),
                ((N_TP, N_EP, CAP, COLS), BF16),
                ((N_TP, N_EP, CAP, COLS), BF16),
                ((N_Z, N_TP, CHUNK, 256), BF16),
                ((N_Z, PER_Z, CAP, COLS), BF16),
                ((N_EP, CAP, COLS), BF16),
                ((512, 128), F32),
                ((512, COLS), F32),
                ((2, N_Z, 4, 160, 256), BF16),
                ((256, 256), BF16),
                ((4, 256, 256), BF16),
                ((256, 1), F32),
                ((256, 1), F32),
                ((256, 256), F32),
                ((N_TP, 32, 2048), BF16),
                ((N_TP, 32, 2048), BF16),
            )
        ]
        + [dma((19,)), dma((24,)), dma((6,)), dma((N_TP,))]
        + [dma((N_Z,))] * 16,
        compiler_params=pltpu.CompilerParams(
            collective_id=0, has_side_effects=True, vmem_limit_bytes=VMEM_LIMIT
        ),
        name="exchange",
    )(
        ffn_gain.reshape(1, -1), route_expert.T, route_weight.T, key_latent, rope_key.T, key_gain.reshape(1, -1),
        query_latent, query_gain.reshape(1, -1), rows, cols,
        tokens_b, w_gate[0], w_up[0], w_down[0], w_query, w_query_rope, w_key, w_value, w_out,
    )

    moe_out, mixer_out = pl.pallas_call(
        finish_kernel,
        out_shape=(struct((512, COLS)), struct((32, 2048))),
        in_specs=[VM] * 2,
        out_specs=(VM, VM),
        compiler_params=pltpu.CompilerParams(vmem_limit_bytes=VMEM_LIMIT),
        name="finish",
    )(moe, mixed)

    return (mixer_out, moe_out)


def solution(mesh):
    in_specs = (
        P("ep", None),
        P("ep", None),
        P("ep", None),
        P(),
        P(),
        P(None, "tp"),
        P(None, "tp"),
        P(None, "tp"),
        P(None, "tp"),
        P("tp", None),
        P("ep", None),
        P(),
        P("ep", None),
        P("ep", None),
        P("ep", None, "tp"),
        P("ep", None, "tp"),
        P("ep", "tp", None),
    )
    out_specs = (P(("ep", "tp"), None), P("ep", "tp"))
    return jax.shard_map(body, mesh=mesh, in_specs=in_specs, out_specs=out_specs, check_vma=False)
```
